256 devices in a mesh: sp: 32 (over z, x), tp: 8 (over y, core).
Axes of the slice: x: 4, y: 4, z: 8, core: 2. Of those that a mesh axis runs over, the one named last changes fastest.
Arguments:
- residual_signal: bfloat16 [4096, 2048], P('sp', 'tp'), may hold values from -90 to 90
- lifted_signal: bfloat16 [4096, 1024], P('sp', 'tp'), may hold values from -6 to 6
- discrete_timestep: float32 [64, 4096], P('tp', 'sp'), may hold values from 0.17 to 4.2
- additional_log_fading: float32 [64, 4096], P('tp', 'sp'), may hold values from -2.1 to 0
- paired_fading: float32 [2, 32, 64], replicated, may hold values from 4.8828125e-06 to 0.0625
- unpaired_fading: float32 [2, 32, 32], replicated, may hold values from 4.8828125e-06 to 0.0625
- paired_twist: float32 [2, 32, 64], replicated, may hold values from -3.140625 to 3.140625
- unpaired_twist: float32 [2, 32, 32], replicated, may hold values from -3.140625 to 3.140625
- paired_latent_linears: float32 [2, 2, 2, 32, 64, 16], replicated, may hold values from -1 to 1
- unpaired_latent_linears: float32 [2, 2, 2, 32, 32, 16], replicated, may hold values from -1 to 1
- skip_coefficient: float32 [1024], replicated, may hold values from -4 to 4
- closing_norm_multiplier: float32 [1024], replicated, may hold values from 0.1 to 1.9
- emitted_linear: bfloat16 [1024, 2048], replicated, may hold values from -0.1875 to 0.1875
- leading_norm_multiplier: float32 [2048], replicated, may hold values from 0.1 to 1.9
- raising_linear: bfloat16 [2048, 8192], P('sp', 'tp'), may hold values from -0.125 to 0.125
- lowering_linear: bfloat16 [8192, 2048], P('tp', 'sp'), may hold values from -0.0625 to 0.0625
Outputs:
- layer_out: bfloat16 [4096, 2048], P('sp', 'tp')
The draws below stay inside these ranges and needn't reach their ends.
All inputs are finite; a program needn't handle non-finite values.
Results may differ from the reference program's by a relative error of at most 0.008.
Values may be sent and summed in bfloat16 or wider, within the bound.
A program may use at most 128 MiB of HBM per device.

```python
import math
import jax
import jax.numpy as jnp
from jax import lax

D = 2048
FF = 8192
MIXER_BANDS = 64
CHAN = 16
STATE_LONG = 64
STATE_SHORT = 32
NORM_W = 128
TOK_DEV = 128
SSM_W = 1024
TOKENS = 4096
N_TP = 8


def draw_residual_signal(key, part):
    keys = jax.random.split(jax.random.fold_in(key, 5), 3)
    column = 0.4 * 10.0 ** (jnp.arange(D, dtype=jnp.float32) / D)
    column = column * jax.random.uniform(keys[0], (D,), jnp.float32, 0.7, 1.4)
    base = jnp.clip(jax.random.normal(keys[1], (TOKENS, D), jnp.float32), -4.0, 4.0)
    row_scale = jnp.exp(jax.random.uniform(keys[2], (TOKENS,), jnp.float32, math.log(0.5), math.log(4.0)))
    return (base * row_scale[:, None] * column[None, :]).astype(jnp.bfloat16)


def draw_discrete_timestep(key, part):
    keys = jax.random.split(jax.random.fold_in(key, 7), 2)
    span = TOK_DEV // 2
    count = TOKENS // span
    lowest, highest, rough_low, rough_high = (0.5, 2.0, 0.5, 1.5)
    factor = jnp.exp(jax.random.uniform(keys[0], (count,), jnp.float32, math.log(lowest), math.log(highest)))
    along = jnp.repeat(factor, span)
    rough = jax.random.uniform(keys[1], (MIXER_BANDS, TOKENS), jnp.float32, rough_low, rough_high)
    return along[None, :] * rough


def draw_additional_log_fading(key, part):
    keys = jax.random.split(jax.random.fold_in(key, 9), 2)
    places = jax.random.randint(keys[0], (MIXER_BANDS, 3), 0, TOKENS)
    values = jax.random.uniform(keys[1], (MIXER_BANDS, 3), jnp.float32, math.log(0.5), math.log(0.8))
    hits = (jnp.arange(TOKENS)[None, None, :] == places[:, :, None]).astype(jnp.float32)
    return jnp.sum(hits * values[:, :, None], axis=1)


def draw_rates(key, states):
    keys = jax.random.split(key, 4)
    share = 8
    quick = jax.random.randint(keys[0], (2, MIXER_BANDS // 2), 0, 16) < share
    quick_rate = jnp.exp(jax.random.uniform(keys[1], (2, MIXER_BANDS // 2), jnp.float32, math.log(0.01), math.log(0.025)))
    slow_rate = jnp.exp(jax.random.uniform(keys[2], (2, MIXER_BANDS // 2), jnp.float32, math.log(0.02), math.log(0.12))) / TOKENS
    base = jnp.where(quick, quick_rate, slow_rate)
    spread = jnp.exp(jax.random.uniform(keys[3], (2, MIXER_BANDS // 2, states), jnp.float32, 0.0, math.log(2.5)))
    return base[:, :, None] * spread


def draw_paired_fading(key, part):
    return draw_rates(jax.random.fold_in(key, 11), STATE_LONG)


def draw_unpaired_fading(key, part):
    return draw_rates(jax.random.fold_in(key, 12), STATE_SHORT)


def level_of(key, dims, cuts, least, high):
    def one(axis_at, parts):
        heights = jax.random.uniform(jax.random.fold_in(jax.random.fold_in(key, 6), axis_at), (parts,), jnp.float32, least / len(cuts), high / len(cuts))
        return jnp.repeat(jnp.exp(heights), dims[axis_at] // parts).reshape((-1,) + (1,) * (len(dims) - axis_at - 1))

    level = one(*cuts[0])
    for cut in cuts[1:]:
        level = level * one(*cut)
    return level


def scatter_about(stream_key, shape, deviation, most, cuts=(), kind=jnp.bfloat16):
    drawn = jax.random.normal(stream_key, shape, jnp.float32) * deviation
    if len(cuts) > 0:
        drawn = level_of(stream_key, shape, cuts, -0.22, 0.18) * drawn
    return jnp.clip(drawn, min=-most, max=most).astype(kind)


def setup_inputs(seed: int = 0) -> dict:
    seeds = jax.random.split(jax.random.key(seed), 17)
    residual_signal = draw_residual_signal(jax.random.fold_in(seeds[16], 71), 0)
    lifted_signal = scatter_about(seeds[1], (TOKENS, SSM_W), 1.0, 6.0, ((0, 32), (1, 8)))
    discrete_timestep = draw_discrete_timestep(jax.random.fold_in(seeds[16], 71), 0)
    additional_log_fading = draw_additional_log_fading(jax.random.fold_in(seeds[16], 71), 0)
    paired_fading = draw_paired_fading(jax.random.fold_in(seeds[16], 71), 0)
    unpaired_fading = draw_unpaired_fading(jax.random.fold_in(seeds[16], 71), 0)
    paired_twist = jnp.clip(jax.random.uniform(seeds[6], (2, MIXER_BANDS // 2, STATE_LONG), jnp.float32, -3.140625, 3.140625), -3.140625, 3.140625)
    unpaired_twist = jnp.clip(jax.random.uniform(seeds[7], (2, MIXER_BANDS // 2, STATE_SHORT), jnp.float32, -3.140625, 3.140625), -3.140625, 3.140625)
    paired_latent_linears = scatter_about(seeds[8], (2, 2, 2, MIXER_BANDS // 2, STATE_LONG, CHAN), (2 * CHAN) ** -0.5, 1.0, (), jnp.float32)
    unpaired_latent_linears = scatter_about(seeds[9], (2, 2, 2, MIXER_BANDS // 2, STATE_SHORT, CHAN), (2 * CHAN) ** -0.5, 1.0, (), jnp.float32)
    skip_coefficient = scatter_about(seeds[10], (SSM_W,), 1.0, 4.0, (), jnp.float32)
    closing_norm_multiplier = jnp.clip(1.0 + 0.18 * jax.random.normal(seeds[11], (SSM_W,), jnp.float32), 0.1, 1.9)
    emitted_linear = scatter_about(seeds[12], (SSM_W, D), SSM_W ** -0.5, 0.1875)
    leading_norm_multiplier = jnp.clip(1.0 + 0.18 * jax.random.normal(seeds[13], (D,), jnp.float32), 0.1, 1.9)
    raising_linear = scatter_about(seeds[14], (D, FF), D ** -0.5, 0.125, ((0, 32), (1, 8)))
    lowering_linear = scatter_about(seeds[15], (FF, D), FF ** -0.5, 0.0625, ((0, 8), (1, 32)))
    return {"residual_signal": residual_signal, "lifted_signal": lifted_signal, "discrete_timestep": discrete_timestep, "additional_log_fading": additional_log_fading, "paired_fading": paired_fading, "unpaired_fading": unpaired_fading, "paired_twist": paired_twist, "unpaired_twist": unpaired_twist, "paired_latent_linears": paired_latent_linears, "unpaired_latent_linears": unpaired_latent_linears, "skip_coefficient": skip_coefficient, "closing_norm_multiplier": closing_norm_multiplier, "emitted_linear": emitted_linear, "leading_norm_multiplier": leading_norm_multiplier, "raising_linear": raising_linear, "lowering_linear": lowering_linear}


EPSILON = 1e-06

def combine_maps(early, later):
    first_re, first_im, base_re, base_im = early
    next_re, next_im, add_re, add_im = later
    return (next_re * first_re - next_im * first_im, next_re * first_im + next_im * first_re, next_re * base_re - next_im * base_im + add_re, next_re * base_im + next_im * base_re + add_im)

def step_maps(group_inputs, pace, surge_entries, decay_rate, turn_rate, input_re, input_im):
    scaled = pace[:, :, None]
    magnitude = jnp.exp(-decay_rate[None] * scaled + surge_entries[:, :, None])
    angle = turn_rate[None] * scaled
    weight_in = jnp.sqrt(-jnp.expm1(-2.0 * decay_rate[None] * scaled))
    drive_re = jnp.einsum('ngj,gpj->ngp', group_inputs, input_re, precision=lax.Precision.HIGHEST) * weight_in
    drive_im = jnp.einsum('ngj,gpj->ngp', group_inputs, input_im, precision=lax.Precision.HIGHEST) * weight_in
    return (magnitude * jnp.cos(angle), magnitude * jnp.sin(angle), drive_re, drive_im)

def readout(state_re, state_im, read_re, read_im):
    return jnp.einsum('ngp,gpj->ngj', state_re, read_re, precision=lax.Precision.HIGHEST) - jnp.einsum('ngp,gpj->ngj', state_im, read_im, precision=lax.Precision.HIGHEST)

def kind_output(group_inputs, pace, surge_entries, decay_rate, turn_rate, projection):
    batch_number = group_inputs.shape[0]
    count = batch_number // TOK_DEV
    width = group_inputs.shape[1]
    states = decay_rate.shape[-1]
    input_blocks = group_inputs.reshape(count, TOK_DEV, width, CHAN)
    pace_blocks = pace.reshape(count, TOK_DEV, width)
    jolt_blocks = surge_entries.reshape(count, TOK_DEV, width)
    result = jnp.zeros((count, TOK_DEV, width, CHAN), jnp.float32)
    for direction in range(2):
        backward = direction == 1
        edge = 0 if backward else -1

        def each_block(carry, pieces, direction=direction, backward=backward, edge=edge):
            block_inputs, block_pace, block_jolts = pieces
            maps = step_maps(block_inputs, block_pace, block_jolts, decay_rate[direction], turn_rate[direction], projection[direction, 0, 0], projection[direction, 0, 1])
            prefix_re, prefix_im, state_re, state_im = lax.associative_scan(combine_maps, maps, reverse=backward, axis=0)
            carry_re, carry_im = carry
            state_re = state_re + prefix_re * carry_re[None] - prefix_im * carry_im[None]
            state_im = state_im + prefix_re * carry_im[None] + prefix_im * carry_re[None]
            values = readout(state_re, state_im, projection[direction, 1, 0], projection[direction, 1, 1])
            return ((state_re[edge], state_im[edge]), values)
        start = (jnp.zeros((width, states), jnp.float32), jnp.zeros((width, states), jnp.float32))
        _, values = lax.scan(each_block, start, (input_blocks, pace_blocks, jolt_blocks), reverse=backward)
        result = result + values
    return result.reshape(batch_number, width, CHAN)

def reference(residual_signal, lifted_signal, discrete_timestep, additional_log_fading, paired_fading, unpaired_fading, paired_twist, unpaired_twist, paired_latent_linears, unpaired_latent_linears, skip_coefficient, closing_norm_multiplier, emitted_linear, leading_norm_multiplier, raising_linear, lowering_linear):
    batch_number = residual_signal.shape[0]
    grouped = lifted_signal.astype(jnp.float32).reshape(batch_number, MIXER_BANDS // 2, 2, CHAN)
    pace = discrete_timestep.T.reshape(batch_number, MIXER_BANDS // 2, 2)
    surge_entries = additional_log_fading.T.reshape(batch_number, MIXER_BANDS // 2, 2)
    long_out = kind_output(grouped[:, :, 0], pace[:, :, 0], surge_entries[:, :, 0], paired_fading, paired_twist, paired_latent_linears)
    short_out = kind_output(grouped[:, :, 1], pace[:, :, 1], surge_entries[:, :, 1], unpaired_fading, unpaired_twist, unpaired_latent_linears)
    ssm_out = jnp.stack([long_out, short_out], axis=2).reshape(batch_number, SSM_W)
    activated = jax.nn.gelu(ssm_out + skip_coefficient[None] * grouped.reshape(batch_number, SSM_W))
    heads = activated.reshape(batch_number, SSM_W // NORM_W, NORM_W)
    heads = heads * lax.rsqrt(lax.optimization_barrier(jnp.mean(heads * heads, axis=2, keepdims=True)) + EPSILON)
    combined_result = (heads.reshape(batch_number, SSM_W) * closing_norm_multiplier[None]).astype(jnp.bfloat16)
    inner_activity = residual_signal.astype(jnp.float32) + jnp.dot(combined_result, emitted_linear, preferred_element_type=jnp.float32)
    scale = lax.rsqrt(lax.optimization_barrier(jnp.mean(inner_activity * inner_activity, axis=1, keepdims=True)) + EPSILON)
    normed = (inner_activity * scale * leading_norm_multiplier[None]).astype(jnp.bfloat16)
    block_width = FF // N_TP
    feed = jnp.zeros((batch_number, D), jnp.float32)
    for member in range(N_TP):
        upward = jnp.dot(normed, raising_linear[:, member * block_width:(member + 1) * block_width], preferred_element_type=jnp.float32)
        hidden = jnp.square(jax.nn.relu(upward)).astype(jnp.bfloat16)
        product = jnp.dot(hidden, lowering_linear[member * block_width:(member + 1) * block_width], preferred_element_type=jnp.float32).astype(jnp.bfloat16)
        feed = feed + product.astype(jnp.float32)
    return (inner_activity + feed).astype(jnp.bfloat16)
```

```python
import jax
import jax.numpy as jnp
from jax import lax
from jax.experimental import pallas as pl
from jax.experimental.pallas import tpu as pltpu
from jax.sharding import PartitionSpec as P

F32 = jnp.float32
BF16 = jnp.bfloat16
HI = lax.Precision.HIGHEST
MESH = pl.DeviceIdType.MESH
EPSILON = 1e-6

NX, NY, NZ = 4, 4, 8
TOK = 128
CH = 128
ST = 384
LONG = 256
D = 2048
STEPS = 16
CHUNKS = 8


def iota(shape, dim):
    return lax.broadcasted_iota(jnp.int32, shape, dim)


def one_hot(pred):
    return jnp.where(pred, 1.0, 0.0).astype(F32)


def nt(a, b, precision=None):
    return lax.dot_general(
        a, b, (((1,), (1,)), ((), ())), precision=precision, preferred_element_type=F32
    )


def mm(a, b, precision=None):
    return jnp.dot(a, b, precision=precision, preferred_element_type=F32)


def sincos(a):
    k = jnp.floor(a * 0.6366197723675814 + 0.5)
    r = ((a - k * 1.5703125) - k * 4.837512969970703125e-4) - k * 7.549789948768648e-8
    z = r * r
    s = ((-1.9515295891e-4 * z + 8.3321608736e-3) * z - 1.6666654611e-1) * z * r + r
    c = ((2.443315711809948e-5 * z - 1.388731625493765e-3) * z + 4.166664568298827e-2) * z * z
    c = c - 0.5 * z + 1.0
    half = jnp.floor(k * 0.5)
    odd = (k - 2.0 * half) > 0.5
    low = half - 2.0 * jnp.floor(half * 0.5)
    sin_sign = 1.0 - 2.0 * low
    cos_sign = jnp.where(odd, -sin_sign, sin_sign)
    return jnp.where(odd, c, s) * sin_sign, jnp.where(odd, s, c) * cos_sign


def lost(u):
    poly = 1.0 - u * (1.0 / 8)
    for n in (7, 6, 5, 4, 3, 2):
        poly = 1.0 - u * poly * (1.0 / n)
    return jnp.where(u < 0.6, u * poly, 1.0 - jnp.exp(-u))


def kernel(
    residual, lifted, pace, fading, rate_l, rate_s, turn_l, turn_s, proj_l, proj_s,
    skip, closing, emitted, leading, raising, lowering,
    out,
    lifted_v, pace_v, fading_v, rate_lv, rate_sv, turn_lv, turn_sv, proj_lv, proj_sv,
    skip_v, closing_v, emitted_v, leading_v,
    maps_v, pace_s, fading_s, drive_s, prefix_s, state_s, lifted_s,
    ends, cx, cz, row_ends, merged_v, gathered, res_v, mid_v, mid_f, own_mid,
    weights, hidden, partial, arrived,
    load_sem, up_send, up_recv, down_send, down_recv, cx_send, cx_recv, cz_send, cz_recv,
    mg_send, mg_recv, rs_send, rs_recv, res_send, res_recv, ring_send, ring_recv,
    sib_send, sib_recv, mid_send, mid_recv,
):
    sp = lax.axis_index("sp")
    tp = lax.axis_index("tp")
    z, x = sp // NX, sp % NX
    y, c = tp // 2, tp % 2
    sib = y * 2 + (1 - c)
    chip = x * NY + y
    block = x // 2
    inner = x % 2

    def remote(src, dst, send, recv, to):
        return pltpu.make_async_remote_copy(
            src_ref=src, dst_ref=dst, send_sem=send, recv_sem=recv,
            device_id=to, device_id_type=MESH,
        )

    def arrival(ref, sem):
        pltpu.make_async_copy(ref, ref, sem).wait()

    barrier = pltpu.get_barrier_semaphore()
    spot = x * 8 + tp

    @pl.loop(1, 32)
    def _(off):
        to = (spot + off) % 32
        pl.semaphore_signal(barrier, inc=1, device_id=(z * NX + to // 8, to % 8), device_id_type=MESH)

    @pl.loop(1, NZ)
    def _(off):
        pl.semaphore_signal(
            barrier, inc=1, device_id=(((z + off) % NZ) * NX + x, tp), device_id_type=MESH
        )

    loads = [
        (lifted, lifted_v), (pace, pace_v), (fading, fading_v), (rate_l, rate_lv),
        (rate_s, rate_sv), (turn_l, turn_lv), (turn_s, turn_sv),
        (proj_l.at[:, :, :, pl.ds(tp * 4, 4)], proj_lv),
        (proj_s.at[:, :, :, pl.ds(tp * 4, 4)], proj_sv),
        (skip, skip_v), (closing, closing_v), (leading, leading_v), (emitted, emitted_v),
    ]
    copies = [pltpu.make_async_copy(a, b, load_sem.at[n]) for n, (a, b) in enumerate(loads)]
    for copy in copies:
        copy.start()
    for copy in copies[:-1]:
        copy.wait()

    r2, t2 = iota((TOK, TOK), 0), iota((TOK, TOK), 1)
    perm = one_hot(t2 == (r2 & 7) * STEPS + (r2 >> 3))
    perm_back = one_hot(r2 == (t2 & 7) * STEPS + (t2 >> 3))
    p8, g8 = iota((8, ST), 1), iota((8, ST), 0)
    group8 = jnp.where(p8 < LONG, (p8 >> 6) * 2, ((p8 - LONG) >> 5) * 2 + 1)
    spread = one_hot(g8 == group8)
    pace_s[...] = mm(nt(perm, pace_v[...], HI), spread, HI)
    fading_s[...] = mm(nt(perm, fading_v[...], HI), spread, HI)
    lifted_p = mm(perm.astype(BF16), lifted_v[...])
    lifted_s[...] = lifted_p

    def flat(long_ref, short_ref, e):
        a = mm(long_ref[e], one_hot(iota((64, LONG), 0) == (iota((64, LONG), 1) & 63)), HI)
        own = iota((32, LONG), 0) == tp * 4 + (iota((32, LONG), 1) >> 6)
        a = jnp.sum(jnp.where(own, a, 0.0), axis=0, keepdims=True)
        b = mm(short_ref[e], one_hot(iota((32, CH), 0) == (iota((32, CH), 1) & 31)), HI)
        own = iota((32, CH), 0) == tp * 4 + (iota((32, CH), 1) >> 5)
        b = jnp.sum(jnp.where(own, b, 0.0), axis=0, keepdims=True)
        return jnp.concatenate([a, b], axis=1)

    rates = [flat(rate_lv, rate_sv, e) for e in range(2)]
    turns = [flat(turn_lv, turn_sv, e) for e in range(2)]

    tile_l = one_hot(iota((64, LONG), 0) == (iota((64, LONG), 1) & 63))
    tile_s = one_hot(iota((32, CH), 0) == (iota((32, CH), 1) & 31))
    own_l = (iota((64, LONG), 0) >> 4) == (iota((64, LONG), 1) >> 6)
    own_s = (iota((64, CH), 0) >> 4) == (iota((64, CH), 1) >> 5)
    maps_v[...] = jnp.zeros(maps_v.shape, F32)
    for e in range(2):
        for io in range(2):
            for part in range(2):
                a = mm(proj_lv[e, io, part].reshape(64, 64), tile_l, HI)
                a = jnp.where(own_l, a, 0.0)
                b = mm(proj_sv[e, io, part].reshape(64, 32), tile_s, HI)
                b = jnp.where(own_s, b, 0.0)
                for n in range(4):
                    rows = slice(16 * n, 16 * n + 16)
                    maps_v[e, io, part, 32 * n : 32 * n + 16, :LONG] = a[rows]
                    maps_v[e, io, part, 32 * n + 16 : 32 * n + 32, LONG:] = b[rows]
    for e in range(2):
        for part in range(2):
            drive_s[e, part] = mm(lifted_p, maps_v[e, 0, part], HI)

    pl.semaphore_wait(barrier, 31 + NZ - 1)

    def pieces(off):
        xt = (x + off) % NX
        up_src = raising.at[:, pl.ds(pl.multiple_of(xt * 256, 256), 256)]
        up_dst = weights.at[0, z, c, pl.ds(x * 64, 64), :]
        down_src = lowering.at[:, pl.ds(pl.multiple_of(xt * 256, 256), 256)]
        down_dst = weights.at[1, z, c, pl.ds(x * 64, 64), :]
        return xt, up_src, up_dst, down_src, down_dst

    sends = []
    for off in (2, 1, 3):
        xt, up_src, up_dst, down_src, down_dst = pieces(off)
        to = (z * NX + xt, tp)
        sends.append(remote(up_src, up_dst, up_send.at[off], up_recv, to))
        sends.append(remote(down_src, down_dst, down_send.at[off], down_recv, to))
    for copy in sends:
        copy.start()
    _, up_src, up_dst, down_src, down_dst = pieces(0)
    pltpu.make_async_copy(up_src, up_dst, up_recv).start()
    pltpu.make_async_copy(down_src, down_dst, down_recv).start()

    def step(s, carry):
        new = []
        for e in range(2):
            rows = pl.ds(pl.multiple_of((s if e == 0 else STEPS - 1 - s) * 8, 8), 8)
            pre, pim, hre, him = carry[4 * e : 4 * e + 4]
            dt = pace_s[rows, :]
            fade = rates[e] * dt
            mag = jnp.exp(fading_s[rows, :] - fade)
            sn, cs = sincos(turns[e] * dt)
            are, aim = mag * cs, mag * sn
            gain = jnp.sqrt(lost(2.0 * fade))
            bre, bim = drive_s[e, 0, rows, :] * gain, drive_s[e, 1, rows, :] * gain
            pre, pim = are * pre - aim * pim, are * pim + aim * pre
            hre, him = are * hre - aim * him + bre, are * him + aim * hre + bim
            prefix_s[e, 0, rows, :] = pre
            prefix_s[e, 1, rows, :] = pim
            state_s[e, 0, rows, :] = hre
            state_s[e, 1, rows, :] = him
            new += [pre, pim, hre, him]
        return tuple(new)

    one, zero = jnp.ones((8, ST), F32), jnp.zeros((8, ST), F32)
    tops = lax.fori_loop(0, STEPS, step, (one, zero, zero, zero) * 2)

    def composed(first, later):
        fre, fim, bre, bim = first
        nre, nim, are, aim = later
        return (
            nre * fre - nim * fim, nre * fim + nim * fre,
            nre * bre - nim * bim + are, nre * bim + nim * bre + aim,
        )

    unit = (jnp.ones((1, ST), F32),) + (jnp.zeros((1, ST), F32),) * 3
    before = []
    totals = []
    for e in range(2):
        run, rows = unit, [None] * CHUNKS
        for n in range(CHUNKS):
            n = n if e == 0 else CHUNKS - 1 - n
            rows[n] = run
            run = composed(run, tuple(m[n : n + 1] for m in tops[4 * e : 4 * e + 4]))
        before.append(tuple(jnp.concatenate([r[q] for r in rows], axis=0) for q in range(4)))
        totals += list(run)
    own_ends = jnp.concatenate(totals, axis=0)
    ends[...] = own_ends
    cx[x] = own_ends
    for off in (1, 3, 2):
        copy = remote(ends, cx.at[x], cx_send.at[off], cx_recv, (z * NX + (x + off) % NX, tp))
        copy.start()
        sends.append(copy)
    arrival(cx.at[pl.ds(0, NX - 1)], cx_recv)

    def as_map(ref, n, e):
        return tuple(ref[n, 4 * e + q : 4 * e + q + 1, :] for q in range(4))

    row = []
    for e in range(2):
        run = unit
        for n in range(NX) if e == 0 else reversed(range(NX)):
            run = composed(run, as_map(cx, n, e))
        row += list(run)
    row_total = jnp.concatenate(row, axis=0)
    row_ends[...] = row_total
    cz[z] = row_total
    for off in (4, 3, 5, 2, 6, 1, 7):
        copy = remote(
            row_ends, cz.at[z], cz_send.at[off], cz_recv, (((z + off) % NZ) * NX + x, tp)
        )
        copy.start()
        sends.append(copy)

    own_block = pl.ds(pl.multiple_of(inner * TOK, TOK), TOK)

    def plane(off):
        to = (chip + off) % (NX * NY)
        return (z * NX + to // NY, (to % NY) * 2 + block)

    def to_plane(src, dst, send, recv):
        @pl.loop(1, NX * NY)
        def _(off):
            remote(src, dst, send.at[off], recv, plane(off)).start()

        @pl.when(c == block)
        def _():
            pltpu.make_async_copy(src, dst, recv).start()

        @pl.when(c != block)
        def _():
            remote(src, dst, send.at[0], recv, plane(0)).start()

    def plane_sent(src, dst, send, recv):
        @pl.loop(1, NX * NY)
        def _(off):
            remote(src, dst, send.at[off], recv, plane(off)).wait_send()

        @pl.when(c != block)
        def _():
            remote(src, dst, send.at[0], recv, plane(0)).wait_send()

    res_dst = res_v.at[own_block, pl.ds(pl.multiple_of(tp * 256, 256), 256)]
    to_plane(residual, res_dst, res_send, res_recv)

    arrival(weights.at[0, z, c], up_recv)
    arrival(weights.at[1, z, c], down_recv)

    def share(kind, zs, slot):
        ref = weights.at[kind, zs, c]
        copy = remote(ref, ref, sib_send.at[slot], sib_recv.at[kind], (sp, sib))
        copy.start()
        sends.append(copy)

    def ring(ref, way, k):
        to = ((z + (1 if way == 0 else NZ - 1)) % NZ) * NX + x
        copy = remote(ref, ref, ring_send.at[way, k], ring_recv.at[way, k], (to, tp))
        copy.start()
        sends.append(copy)

    def kind_of(way, k):
        return k % 2 if way == 0 else 1 - k % 2

    for k in range(2):
        for way in range(2):
            ring(weights.at[kind_of(way, k), z, c], way, k)
    for kind in range(2):
        share(kind, z, kind)

    def ring_step(k):
        for way in range(2):
            hops = k // 2 + 1
            zs = (z + (NZ - hops if way == 0 else hops)) % NZ
            kind = kind_of(way, k)
            ref = weights.at[kind, zs, c]
            arrival(ref, ring_recv.at[way, k])
            if k < 5:
                ring(ref, way, k + 2)
            share(kind, zs, 2 + 2 * k + way)

    arrival(cz.at[pl.ds(0, NZ - 1)], cz_recv)

    def applied(m, state):
        pre, pim, hre, him = m
        re, im = state
        return pre * re - pim * im + hre, pre * im + pim * re + him

    blank = jnp.zeros((1, ST), F32)
    out_y = jnp.zeros((TOK, CH), F32)
    for e in range(2):
        state = (blank, blank)
        for ref, count, at in ((cz, NZ, z), (cx, NX, x)):
            for n in range(count) if e == 0 else reversed(range(count)):
                passed = (n < at) if e == 0 else (n > at)
                new = applied(as_map(ref, n, e), state)
                state = tuple(jnp.where(passed, a, b) for a, b in zip(new, state))
        entry = applied(before[e], state)
        tall = tuple(jnp.concatenate([v] * STEPS, axis=0) for v in entry)
        pre, pim = prefix_s[e, 0], prefix_s[e, 1]
        re = state_s[e, 0] + pre * tall[0] - pim * tall[1]
        im = state_s[e, 1] + pre * tall[1] + pim * tall[0]
        out_y = out_y + nt(re, maps_v[e, 1, 0], HI) - nt(im, maps_v[e, 1, 1], HI)

    mine = iota((8, CH), 0) == tp
    skip_row = jnp.sum(jnp.where(mine, skip_v[...], 0.0), axis=0, keepdims=True)
    closing_row = jnp.sum(jnp.where(mine, closing_v[...], 0.0), axis=0, keepdims=True)
    v = out_y + skip_row * lifted_s[...]
    act = 0.5 * v * (1.0 + jnp.tanh(0.7978845608028654 * (v + 0.044715 * v * v * v)))
    act = act * lax.rsqrt(jnp.mean(act * act, axis=1, keepdims=True) + EPSILON) * closing_row
    merged_v[...] = mm(perm_back.astype(BF16), act.astype(BF16)).astype(BF16)
    mg_dst = gathered.at[own_block, pl.ds(pl.multiple_of(tp * CH, CH), CH)]
    to_plane(merged_v, mg_dst, mg_send, mg_recv)

    for k in range(4):
        ring_step(k)
    copies[-1].wait()
    arrival(res_v, res_recv)
    arrival(gathered, mg_recv)

    def project(n, squares):
        cols = pl.ds(pl.multiple_of(n * 256, 256), 256)
        m = mm(gathered[...], emitted_v[:, cols]) + res_v[:, cols].astype(F32)
        mid_f[:, cols] = m
        mid_v[:, cols] = (m * leading_v[:, cols]).astype(BF16)
        return squares + jnp.sum(m * m, axis=1, keepdims=True)

    squares = lax.fori_loop(0, 8, project, jnp.zeros((2 * TOK, 1), F32))
    scale = lax.rsqrt(squares * (1.0 / D) + EPSILON)

    own_cols = pl.ds(pl.multiple_of(tp * 256, 256), 256)
    sib_cols = pl.ds(pl.multiple_of(sib * 256, 256), 256)

    @pl.when(c == block)
    def _():
        remote(mid_f.at[own_block, sib_cols], own_mid, mid_send, mid_recv, (sp, sib)).start()

    for k in range(4, 7):
        ring_step(k)

    arrival(weights.at[0, :, 1 - c], sib_recv.at[0])
    for n in range(2):
        up = mm(mid_v[...], weights[0, :, n].reshape(D, 256)) * scale
        up = jnp.maximum(up, 0.0)
        hidden[:, n * 256 : (n + 1) * 256] = (up * up).astype(BF16)
    arrival(weights.at[1, :, 1 - c], sib_recv.at[1])

    def down(n):
        both = nt(hidden[:, :256], weights[1, n, 0]) + nt(hidden[:, 256:], weights[1, n, 1])
        partial[n] = both.astype(BF16)

    def part(n, i):
        return remote(
            partial.at[n, pl.ds(i * TOK, TOK), :], arrived.at[chip],
            rs_send.at[n, i], rs_recv, (z * NX + 2 * c + i, n),
        )

    @pl.loop(1, 8)
    def _(off):
        n = (tp + off) % 8
        down(n)
        for i in range(2):
            part(n, i).start()

    down(tp)
    for i in range(2):
        here = (2 * c + i) == x

        @pl.when(here)
        def _():
            pltpu.make_async_copy(
                partial.at[tp, pl.ds(i * TOK, TOK), :], arrived.at[chip], rs_recv
            ).start()

        @pl.when(jnp.logical_not(here))
        def _():
            part(tp, i).start()

    @pl.when(c == block)
    def _():
        own_mid_copy = pltpu.make_async_copy(mid_f.at[own_block, own_cols], own_mid, mid_recv)
        own_mid_copy.start()

    arrival(own_mid, mid_recv)
    arrival(arrived, rs_recv)
    total = own_mid[...]
    for n in range(NX * NY):
        total = total + arrived[n].astype(F32)
    out[...] = total.astype(BF16)

    for copy in sends:
        copy.wait_send()
    plane_sent(residual, res_dst, res_send, res_recv)
    plane_sent(merged_v, mg_dst, mg_send, mg_recv)

    @pl.when(c == block)
    def _():
        remote(mid_f.at[own_block, sib_cols], own_mid, mid_send, mid_recv, (sp, sib)).wait_send()

    @pl.loop(1, 8)
    def _(off):
        for i in range(2):
            part((tp + off) % 8, i).wait_send()

    for i in range(2):

        @pl.when((2 * c + i) != x)
        def _():
            part(tp, i).wait_send()


def on_device(
    residual, lifted, pace, fading, rate_l, rate_s, turn_l, turn_s, proj_l, proj_s,
    skip, closing, emitted, leading, raising, lowering,
):
    dma = pltpu.SemaphoreType.DMA
    vm = pltpu.VMEM
    return pl.pallas_call(
        kernel,
        out_shape=jax.ShapeDtypeStruct((TOK, 256), BF16),
        in_specs=[pl.BlockSpec(memory_space=pl.ANY)] * 16,
        out_specs=pl.BlockSpec(memory_space=pltpu.VMEM),
        scratch_shapes=[
            vm((TOK, CH), BF16), vm((8, TOK), F32), vm((8, TOK), F32),
            vm((2, 32, 64), F32), vm((2, 32, 32), F32), vm((2, 32, 64), F32), vm((2, 32, 32), F32),
            vm((2, 2, 2, 4, 16, 64), F32), vm((2, 2, 2, 4, 16, 32), F32),
            vm((8, CH), F32), vm((8, CH), F32), vm((1024, D), BF16), vm((1, D), F32),
            vm((2, 2, 2, CH, ST), F32), vm((TOK, ST), F32), vm((TOK, ST), F32),
            vm((2, 2, TOK, ST), F32), vm((2, 2, TOK, ST), F32), vm((2, 2, TOK, ST), F32),
            vm((TOK, CH), F32),
            vm((8, ST), F32), vm((NX, 8, ST), F32), vm((NZ, 8, ST), F32), vm((8, ST), F32),
            vm((TOK, CH), BF16), vm((2 * TOK, 1024), BF16), vm((2 * TOK, D), BF16),
            vm((2 * TOK, D), BF16), vm((2 * TOK, D), F32), vm((TOK, 256), F32),
            vm((2, NZ, 2, 256, 256), BF16), vm((2 * TOK, 512), BF16),
            vm((8, 2 * TOK, 256), BF16), vm((NX * NY, TOK, 256), BF16),
            dma((13,)), dma((NX,)), dma, dma((NX,)), dma, dma((NX,)), dma, dma((NZ,)), dma,
            dma((16,)), dma, dma((8, 2)), dma, dma((16,)), dma, dma((2, 7)), dma((2, 7)),
            dma((16,)), dma((2,)), dma, dma,
        ],
        compiler_params=pltpu.CompilerParams(
            collective_id=0, has_side_effects=True, vmem_limit_bytes=60 * 1024 * 1024
        ),
        name="layer",
    )(
        residual, lifted, pace, fading, rate_l, rate_s, turn_l, turn_s,
        proj_l.swapaxes(-1, -2), proj_s.swapaxes(-1, -2),
        skip.reshape(8, CH), closing.reshape(8, CH), emitted, leading.reshape(1, D), raising, lowering.T,
    )


def solution(mesh):
    rest = [P()] * 10
    return jax.shard_map(
        on_device,
        mesh=mesh,
        in_specs=(P("sp", "tp"), P("sp", "tp"), P("tp", "sp"), P("tp", "sp"), *rest, P("sp", "tp"), P("tp", "sp")),
        out_specs=P("sp", "tp"),
        check_vma=False,
    )
```

```python
import jax
import jax.numpy as jnp
from jax import lax
from jax.experimental import pallas as pl
from jax.experimental.pallas import tpu as pltpu
from jax.sharding import PartitionSpec as P

F32 = jnp.float32
BF16 = jnp.bfloat16
HI = lax.Precision.HIGHEST
MESH = pl.DeviceIdType.MESH
EPSILON = 1e-6

NX, NY, NZ = 4, 4, 8
TOK = 128
CH = 128
ST = 384
LONG = 256
D = 2048
STEPS = 16
CHUNKS = 8


def iota(shape, dim):
    return lax.broadcasted_iota(jnp.int32, shape, dim)


def one_hot(pred):
    return jnp.where(pred, 1.0, 0.0).astype(F32)


def nt(a, b, precision=None):
    return lax.dot_general(
        a, b, (((1,), (1,)), ((), ())), precision=precision, preferred_element_type=F32
    )


def mm(a, b, precision=None):
    return jnp.dot(a, b, precision=precision, preferred_element_type=F32)


def halves(a):
    high = a.astype(BF16)
    return high, (a - high.astype(F32)).astype(BF16)


def sincos(a):
    k = jnp.floor(a * 0.6366197723675814 + 0.5)
    r = ((a - k * 1.5703125) - k * 4.837512969970703125e-4) - k * 7.549789948768648e-8
    z = r * r
    s = ((-1.9515295891e-4 * z + 8.3321608736e-3) * z - 1.6666654611e-1) * z * r + r
    c = ((2.443315711809948e-5 * z - 1.388731625493765e-3) * z + 4.166664568298827e-2) * z * z
    c = c - 0.5 * z + 1.0
    half = jnp.floor(k * 0.5)
    odd = (k - 2.0 * half) > 0.5
    low = half - 2.0 * jnp.floor(half * 0.5)
    sin_sign = 1.0 - 2.0 * low
    cos_sign = jnp.where(odd, -sin_sign, sin_sign)
    return jnp.where(odd, c, s) * sin_sign, jnp.where(odd, s, c) * cos_sign


def lost(u):
    poly = 1.0 - u * (1.0 / 8)
    for n in (7, 6, 5, 4, 3, 2):
        poly = 1.0 - u * poly * (1.0 / n)
    return jnp.where(u < 0.6, u * poly, 1.0 - jnp.exp(-u))


def kernel(
    residual, lifted, pace, fading, rate_l, rate_s, turn_l, turn_s, proj_l, proj_s,
    skip, closing, emitted, leading, raising, lowering,
    out,
    lifted_v, pace_v, fading_v, rate_lv, rate_sv, turn_lv, turn_sv, proj_lv, proj_sv,
    skip_v, closing_v, raising_v, lowering_v, emitted_v, leading_v,
    maps_v, pace_s, fading_s, drive_s, prefix_s, state_s, lifted_s,
    ends, cx, cz, row_ends, merged_v, gathered, res_v, mid_v, mid_f, own_mid,
    weights, hidden, partial, from_y, from_x, sum_y, sum_x, final,
    load_sem, up_send, up_recv, down_send, down_recv, cx_send, cx_recv, cz_send, cz_recv,
    mg_send, mg_recv, ay_send, ay_recv, ax_send, ax_recv, fy_send, fx_send, final_recv, res_send, res_recv, ring_send, ring_recv,
    sib_send, sib_recv, mid_send, mid_recv,
):
    sp = lax.axis_index("sp")
    tp = lax.axis_index("tp")
    z, x = sp // NX, sp % NX
    y, c = tp // 2, tp % 2
    sib = y * 2 + (1 - c)
    chip = x * NY + y
    block = x // 2
    inner = x % 2

    def remote(src, dst, send, recv, to):
        return pltpu.make_async_remote_copy(
            src_ref=src, dst_ref=dst, send_sem=send, recv_sem=recv,
            device_id=to, device_id_type=MESH,
        )

    def arrival(ref, sem):
        pltpu.make_async_copy(ref, ref, sem).wait()

    barrier = pltpu.get_barrier_semaphore()
    spot = x * 8 + tp

    @pl.loop(1, 32)
    def _(off):
        to = (spot + off) % 32
        pl.semaphore_signal(barrier, inc=1, device_id=(z * NX + to // 8, to % 8), device_id_type=MESH)

    @pl.loop(1, NZ)
    def _(off):
        pl.semaphore_signal(
            barrier, inc=1, device_id=(((z + off) % NZ) * NX + x, tp), device_id_type=MESH
        )

    loads = [
        (lifted, lifted_v), (pace, pace_v), (fading, fading_v), (rate_l, rate_lv),
        (rate_s, rate_sv), (turn_l, turn_lv), (turn_s, turn_sv),
        (proj_l.at[:, :, :, pl.ds(tp * 4, 4)], proj_lv),
        (proj_s.at[:, :, :, pl.ds(tp * 4, 4)], proj_sv),
        (skip, skip_v), (closing, closing_v), (raising, raising_v), (lowering, lowering_v),
        (leading, leading_v), (emitted, emitted_v),
    ]
    copies = [pltpu.make_async_copy(a, b, load_sem.at[n]) for n, (a, b) in enumerate(loads)]
    for copy in copies:
        copy.start()
    for copy in copies[:-4]:
        copy.wait()

    r2, t2 = iota((TOK, TOK), 0), iota((TOK, TOK), 1)
    perm = one_hot(t2 == (r2 & 7) * STEPS + (r2 >> 3))
    perm_back = one_hot(r2 == (t2 & 7) * STEPS + (t2 >> 3))
    p8, g8 = iota((8, ST), 1), iota((8, ST), 0)
    group8 = jnp.where(p8 < LONG, (p8 >> 6) * 2, ((p8 - LONG) >> 5) * 2 + 1)
    spread = one_hot(g8 == group8)
    pace_s[...] = mm(nt(perm, pace_v[...], HI), spread, HI)
    fading_s[...] = mm(nt(perm, fading_v[...], HI), spread, HI)
    lifted_p = mm(perm.astype(BF16), lifted_v[...])
    lifted_s[...] = lifted_p

    def flat(long_ref, short_ref, e):
        a = mm(long_ref[e], one_hot(iota((64, LONG), 0) == (iota((64, LONG), 1) & 63)), HI)
        own = iota((32, LONG), 0) == tp * 4 + (iota((32, LONG), 1) >> 6)
        a = jnp.sum(jnp.where(own, a, 0.0), axis=0, keepdims=True)
        b = mm(short_ref[e], one_hot(iota((32, CH), 0) == (iota((32, CH), 1) & 31)), HI)
        own = iota((32, CH), 0) == tp * 4 + (iota((32, CH), 1) >> 5)
        b = jnp.sum(jnp.where(own, b, 0.0), axis=0, keepdims=True)
        return jnp.concatenate([a, b], axis=1)

    rates = [flat(rate_lv, rate_sv, e) for e in range(2)]
    turns = [flat(turn_lv, turn_sv, e) for e in range(2)]

    tile_l = one_hot(iota((64, LONG), 0) == (iota((64, LONG), 1) & 63)).astype(BF16)
    tile_s = one_hot(iota((32, CH), 0) == (iota((32, CH), 1) & 31)).astype(BF16)
    own_l = (iota((64, LONG), 0) >> 4) == (iota((64, LONG), 1) >> 6)
    own_s = (iota((64, CH), 0) >> 4) == (iota((64, CH), 1) >> 5)
    maps_v[...] = jnp.zeros(maps_v.shape, BF16)
    for e in range(2):
        for io in range(2):
            for part in range(2):
                wide = halves(proj_lv[e, io, part].reshape(64, 64))
                slim = halves(proj_sv[e, io, part].reshape(64, 32))
                for h in range(2):
                    a = jnp.where(own_l, mm(wide[h], tile_l), 0.0).astype(BF16)
                    b = jnp.where(own_s, mm(slim[h], tile_s), 0.0).astype(BF16)
                    for n in range(4):
                        rows = slice(16 * n, 16 * n + 16)
                        maps_v[e, io, part, h, 32 * n : 32 * n + 16, :LONG] = a[rows]
                        maps_v[e, io, part, h, 32 * n + 16 : 32 * n + 32, LONG:] = b[rows]
    lifted_b = lifted_p.astype(BF16)
    for e in range(2):
        for part in range(2):
            drive_s[e, part] = mm(lifted_b, maps_v[e, 0, part, 0]) + mm(lifted_b, maps_v[e, 0, part, 1])

    copies[-4].wait()
    copies[-3].wait()
    pl.semaphore_wait(barrier, 31 + NZ - 1)

    sends = []

    def begin(copy):
        copy.start()
        sends.append(copy)

    def pieces(off):
        xt = (x + off) % NX
        up_src = raising_v.at[:, pl.ds(pl.multiple_of(xt * 256, 256), 256)]
        up_dst = weights.at[0, z, c, pl.ds(x * 64, 64), :]
        down_src = lowering_v.at[:, pl.ds(pl.multiple_of(xt * 256, 256), 256)]
        down_dst = weights.at[1, z, c, pl.ds(x * 64, 64), :]
        return xt, up_src, up_dst, down_src, down_dst

    for off in (2, 1, 3):
        xt, src, dst, _, _ = pieces(off)
        begin(remote(src, dst, up_send.at[off], up_recv, (z * NX + xt, tp)))
    for off in (2, 1, 3):
        xt, _, _, src, dst = pieces(off)
        begin(remote(src, dst, down_send.at[off], down_recv, (z * NX + xt, tp)))
    _, up_src, up_dst, down_src, down_dst = pieces(0)
    pltpu.make_async_copy(up_src, up_dst, up_recv).start()
    pltpu.make_async_copy(down_src, down_dst, down_recv).start()

    def step(s, carry):
        new = []
        for e in range(2):
            rows = pl.ds(pl.multiple_of((s if e == 0 else STEPS - 1 - s) * 8, 8), 8)
            pre, pim, hre, him = carry[4 * e : 4 * e + 4]
            dt = pace_s[rows, :]
            fade = rates[e] * dt
            mag = jnp.exp(fading_s[rows, :] - fade)
            sn, cs = sincos(turns[e] * dt)
            are, aim = mag * cs, mag * sn
            gain = jnp.sqrt(lost(2.0 * fade))
            bre, bim = drive_s[e, 0, rows, :] * gain, drive_s[e, 1, rows, :] * gain
            pre, pim = are * pre - aim * pim, are * pim + aim * pre
            hre, him = are * hre - aim * him + bre, are * him + aim * hre + bim
            prefix_s[e, 0, rows, :] = pre
            prefix_s[e, 1, rows, :] = pim
            state_s[e, 0, rows, :] = hre
            state_s[e, 1, rows, :] = him
            new += [pre, pim, hre, him]
        return tuple(new)

    one, zero = jnp.ones((8, ST), F32), jnp.zeros((8, ST), F32)
    tops = lax.fori_loop(0, STEPS, step, (one, zero, zero, zero) * 2)

    def composed(first, later):
        fre, fim, bre, bim = first
        nre, nim, are, aim = later
        return (
            nre * fre - nim * fim, nre * fim + nim * fre,
            nre * bre - nim * bim + are, nre * bim + nim * bre + aim,
        )

    unit = (jnp.ones((1, ST), F32),) + (jnp.zeros((1, ST), F32),) * 3
    before = []
    totals = []
    for e in range(2):
        run, rows = unit, [None] * CHUNKS
        for n in range(CHUNKS):
            n = n if e == 0 else CHUNKS - 1 - n
            rows[n] = run
            run = composed(run, tuple(m[n : n + 1] for m in tops[4 * e : 4 * e + 4]))
        before.append(tuple(jnp.concatenate([r[q] for r in rows], axis=0) for q in range(4)))
        totals += list(run)
    own_ends = jnp.concatenate(totals, axis=0)
    ends[...] = own_ends
    cx[x] = own_ends

    for off in (2, 1, 3):
        copy = remote(ends, cx.at[x], cx_send.at[off], cx_recv, (z * NX + (x + off) % NX, tp))
        copy.start()
        sends.append(copy)
    ORDER = (
        (0, 0, 0), (0, 1, 0), (1, 0, 0), (0, 0, 1), (0, 1, 1), (1, 1, 0), (0, 0, 2),
        (0, 1, 2), (1, 0, 1), (0, 0, 3), (1, 1, 1), (1, 0, 2), (1, 1, 2), (1, 0, 3),
    )

    def piece(way, slot, extra):
        kind, half, hops = ORDER[slot]
        hops = hops + extra
        zs = (z + (NZ - hops if way == 0 else hops)) % NZ
        return kind, weights.at[kind, zs, c, pl.ds((half ^ way) * 128, 128), :]

    def share(kind, ref, slot):
        begin(remote(ref, ref, sib_send.at[slot], sib_recv.at[kind], (sp, sib)))

    def ring_send_slot(slot):
        for way in range(2):
            to = ((z + (1 if way == 0 else NZ - 1)) % NZ) * NX + x
            _, ref = piece(way, slot, 0)
            begin(remote(ref, ref, ring_send.at[way, slot], ring_recv.at[way, slot], (to, tp)))

    def ring_take(slot):
        for way in range(2):
            kind, ref = piece(way, slot, 1)
            arrival(ref, ring_recv.at[way, slot])
            share(kind, ref, 2 + 2 * slot + way)

    own_block = pl.ds(pl.multiple_of(inner * TOK, TOK), TOK)

    def plane(off):
        to = (chip + off) % (NX * NY)
        return (z * NX + to // NY, (to % NY) * 2 + block)

    def to_plane(src, dst, send, recv):
        @pl.loop(1, NX * NY)
        def _(off):
            remote(src, dst, send.at[off], recv, plane(off)).start()

        @pl.when(c == block)
        def _():
            pltpu.make_async_copy(src, dst, recv).start()

        @pl.when(c != block)
        def _():
            remote(src, dst, send.at[0], recv, plane(0)).start()

    def plane_sent(src, dst, send, recv):
        @pl.loop(1, NX * NY)
        def _(off):
            remote(src, dst, send.at[off], recv, plane(off)).wait_send()

        @pl.when(c != block)
        def _():
            remote(src, dst, send.at[0], recv, plane(0)).wait_send()

    res_dst = res_v.at[own_block, pl.ds(pl.multiple_of(tp * 256, 256), 256)]
    arrival(weights.at[0, z, c], up_recv)
    ring_send_slot(0)
    ring_send_slot(1)
    share(0, weights.at[0, z, c], 0)
    arrival(cx.at[pl.ds(0, NX - 1)], cx_recv)

    def as_map(ref, n, e):
        return tuple(ref[n, 4 * e + q : 4 * e + q + 1, :] for q in range(4))

    row = []
    for e in range(2):
        run = unit
        for n in range(NX) if e == 0 else reversed(range(NX)):
            run = composed(run, as_map(cx, n, e))
        row += list(run)
    row_total = jnp.concatenate(row, axis=0)
    row_ends[...] = row_total
    cz[z] = row_total
    for off in (4, 3, 5, 2, 6, 1, 7):
        copy = remote(
            row_ends, cz.at[z], cz_send.at[off], cz_recv, (((z + off) % NZ) * NX + x, tp)
        )
        copy.start()
        sends.append(copy)

    arrival(weights.at[1, z, c], down_recv)
    ring_send_slot(2)
    share(1, weights.at[1, z, c], 1)
    to_plane(residual, res_dst, res_send, res_recv)

    ring_take(0)
    ring_send_slot(3)
    ring_take(1)
    ring_send_slot(4)
    ring_send_slot(5)

    arrival(cz.at[pl.ds(0, NZ - 1)], cz_recv)

    def applied(m, state):
        pre, pim, hre, him = m
        re, im = state
        return pre * re - pim * im + hre, pre * im + pim * re + him

    blank = jnp.zeros((1, ST), F32)
    out_y = jnp.zeros((TOK, CH), F32)
    for e in range(2):
        state = (blank, blank)
        for ref, count, at in ((cz, NZ, z), (cx, NX, x)):
            for n in range(count) if e == 0 else reversed(range(count)):
                passed = (n < at) if e == 0 else (n > at)
                new = applied(as_map(ref, n, e), state)
                state = tuple(jnp.where(passed, a, b) for a, b in zip(new, state))
        entry = applied(before[e], state)
        tall = tuple(jnp.concatenate([v] * STEPS, axis=0) for v in entry)
        pre, pim = prefix_s[e, 0], prefix_s[e, 1]
        re = state_s[e, 0] + pre * tall[0] - pim * tall[1]
        im = state_s[e, 1] + pre * tall[1] + pim * tall[0]
        for part, value in ((0, re), (1, -im)):
            high, low = halves(value)
            out_y = out_y + nt(high, maps_v[e, 1, part, 0])
            out_y = out_y + (nt(low, maps_v[e, 1, part, 0]) + nt(high, maps_v[e, 1, part, 1]))

    mine = iota((8, CH), 0) == tp
    skip_row = jnp.sum(jnp.where(mine, skip_v[...], 0.0), axis=0, keepdims=True)
    closing_row = jnp.sum(jnp.where(mine, closing_v[...], 0.0), axis=0, keepdims=True)
    v = out_y + skip_row * lifted_s[...]
    act = 0.5 * v * (1.0 + jnp.tanh(0.7978845608028654 * (v + 0.044715 * v * v * v)))
    act = act * lax.rsqrt(jnp.mean(act * act, axis=1, keepdims=True) + EPSILON) * closing_row
    merged_v[...] = mm(perm_back.astype(BF16), act.astype(BF16)).astype(BF16)
    mg_dst = gathered.at[own_block, pl.ds(pl.multiple_of(tp * CH, CH), CH)]
    to_plane(merged_v, mg_dst, mg_send, mg_recv)

    ring_take(2)
    ring_take(3)
    ring_send_slot(6)
    ring_take(4)
    ring_send_slot(7)
    ring_send_slot(8)
    ring_take(5)
    ring_take(6)
    ring_send_slot(9)
    ring_send_slot(10)
    ring_take(7)
    ring_take(8)
    ring_send_slot(11)
    ring_take(9)
    ring_take(10)
    ring_send_slot(12)
    ring_take(11)
    ring_send_slot(13)
    copies[-1].wait()
    copies[-2].wait()
    arrival(res_v, res_recv)
    ring_take(12)
    arrival(gathered, mg_recv)

    def project(n, squares):
        cols = pl.ds(pl.multiple_of(n * 512, 512), 512)
        m = mm(gathered[...], emitted_v[:, cols]) + res_v[:, cols].astype(F32)
        mid_f[:, cols] = m
        mid_v[:, cols] = (m * leading_v[:, cols]).astype(BF16)
        return squares + jnp.sum(m * m, axis=1, keepdims=True)

    squares = lax.fori_loop(0, 2, project, jnp.zeros((2 * TOK, 1), F32))
    ring_take(13)
    squares = lax.fori_loop(2, 4, project, squares)
    scale = lax.rsqrt(squares * (1.0 / D) + EPSILON)

    own_cols = pl.ds(pl.multiple_of(tp * 256, 256), 256)
    sib_cols = pl.ds(pl.multiple_of(sib * 256, 256), 256)

    @pl.when(c == block)
    def _():
        remote(mid_f.at[own_block, sib_cols], own_mid, mid_send, mid_recv, (sp, sib)).start()

    arrival(weights.at[0, :, 1 - c], sib_recv.at[0])
    for n in range(2):
        up = mm(mid_v[...], weights[0, :, n].reshape(D, 256)) * scale
        up = jnp.maximum(up, 0.0)
        hidden[:, n * 256 : (n + 1) * 256] = (up * up).astype(BF16)
    arrival(weights.at[1, :, 1 - c], sib_recv.at[1])

    def down(n):
        both = nt(hidden[:, :256], weights[1, n, 0]) + nt(hidden[:, 256:], weights[1, n, 1])
        partial[n] = both.astype(BF16)

    def row_of(k):
        return (y + 1 + k) % NY

    def along_y(i, k):
        to = row_of(k)
        src = partial.at[2 * to + 1, pl.ds(i * TOK, TOK), :]
        dst = from_y.at[i, y]
        return src, dst, remote(src, dst, ay_send.at[i, k], ay_recv.at[i], (sp, 2 * to + c))

    def along_x(k, i):
        src = partial.at[2 * row_of(k), pl.ds(i * TOK, TOK), :]
        dst = from_x.at[row_of(k), x]
        to = (z * NX + 2 * c + i, tp)
        return src, dst, remote(src, dst, ax_send.at[k, i], ax_recv.at[k], to)

    def on_y(i):
        dst = final.at[x]
        to = (z * NX + 2 * c + i, y * 2 + 1)
        return sum_y.at[i], dst, remote(sum_y.at[i], dst, fy_send.at[i], final_recv, to)

    def on_x(k):
        dst = final.at[y]
        to = (sp, row_of(k) * 2)
        return sum_x.at[k], dst, remote(sum_x.at[k], dst, fx_send.at[k], final_recv, to)

    def deliver(triple, recv, local):
        src, dst, copy = triple
        if local is None:
            copy.start()
            return

        @pl.when(local)
        def _():
            pltpu.make_async_copy(src, dst, recv).start()

        @pl.when(jnp.logical_not(local))
        def _():
            copy.start()

    def delivered(triple, local):
        if local is None:
            triple[2].wait_send()
            return

        @pl.when(jnp.logical_not(local))
        def _():
            triple[2].wait_send()

    def near(i):
        return (2 * c + i) == x

    def local_y(k):
        return (c == 0) if k == NY - 1 else None

    for k in range(NY):
        down(2 * row_of(k) + 1)
        if k < NY - 1:
            along_y(0, k)[2].start()
        else:
            for i in range(2):
                src, dst, _ = along_y(i, k)
                pltpu.make_async_copy(src, dst, ay_recv.at[i]).start()
        down(2 * row_of(k))
        for i in range(2):
            deliver(along_x(k, i), ax_recv.at[k], near(i))
    for k in range(NY - 1):
        along_y(1, k)[2].start()

    def summed(ref):
        total = ref[0].astype(F32)
        for n in range(1, NX):
            total = total + ref[n].astype(F32)
        return total

    def turn_x(k):
        @pl.when(c == block)
        def _():
            arrival(from_x.at[row_of(k)], ax_recv.at[k])
            sum_x[k] = summed(from_x.at[row_of(k)]).astype(BF16)
            deliver(on_x(k), final_recv, local_y(k))

    def turn_y(i):
        arrival(from_y.at[i], ay_recv.at[i])
        sum_y[i] = summed(from_y.at[i]).astype(BF16)
        deliver(on_y(i), final_recv, jnp.logical_and(near(i), c == 1))

    @pl.when(c == block)
    def _():
        own_mid_copy = pltpu.make_async_copy(mid_f.at[own_block, own_cols], own_mid, mid_recv)
        own_mid_copy.start()

    turn_x(0)
    turn_y(0)
    turn_x(1)
    turn_x(2)
    turn_x(3)
    turn_y(1)

    for copy in sends:
        copy.wait_send()
    plane_sent(residual, res_dst, res_send, res_recv)
    plane_sent(merged_v, mg_dst, mg_send, mg_recv)

    @pl.when(c == block)
    def _():
        remote(mid_f.at[own_block, sib_cols], own_mid, mid_send, mid_recv, (sp, sib)).wait_send()

    arrival(own_mid, mid_recv)
    arrival(final, final_recv)
    out[...] = (own_mid[...] + summed(final)).astype(BF16)

    for k in range(NY):
        for i in range(2):
            delivered(along_x(k, i), near(i))
            if k < NY - 1:
                along_y(i, k)[2].wait_send()

        @pl.when(c == block)
        def _():
            delivered(on_x(k), local_y(k))

    for i in range(2):
        delivered(on_y(i), jnp.logical_and(near(i), c == 1))


def on_device(
    residual, lifted, pace, fading, rate_l, rate_s, turn_l, turn_s, proj_l, proj_s,
    skip, closing, emitted, leading, raising, lowering,
):
    dma = pltpu.SemaphoreType.DMA
    vm = pltpu.VMEM
    return pl.pallas_call(
        kernel,
        out_shape=jax.ShapeDtypeStruct((TOK, 256), BF16),
        in_specs=[pl.BlockSpec(memory_space=pl.ANY)] * 16,
        out_specs=pl.BlockSpec(memory_space=pltpu.VMEM),
        scratch_shapes=[
            vm((TOK, CH), BF16), vm((8, TOK), F32), vm((8, TOK), F32),
            vm((2, 32, 64), F32), vm((2, 32, 32), F32), vm((2, 32, 64), F32), vm((2, 32, 32), F32),
            vm((2, 2, 2, 4, 16, 64), F32), vm((2, 2, 2, 4, 16, 32), F32),
            vm((8, CH), F32), vm((8, CH), F32), vm((64, 1024), BF16), vm((64, 1024), BF16), vm((1024, D), BF16), vm((1, D), F32),
            vm((2, 2, 2, 2, CH, ST), BF16), vm((TOK, ST), F32), vm((TOK, ST), F32),
            vm((2, 2, TOK, ST), F32), vm((2, 2, TOK, ST), F32), vm((2, 2, TOK, ST), F32),
            vm((TOK, CH), F32),
            vm((8, ST), F32), vm((NX, 8, ST), F32), vm((NZ, 8, ST), F32), vm((8, ST), F32),
            vm((TOK, CH), BF16), vm((2 * TOK, 1024), BF16), vm((2 * TOK, D), BF16),
            vm((2 * TOK, D), BF16), vm((2 * TOK, D), F32), vm((TOK, 256), F32),
            vm((2, NZ, 2, 256, 256), BF16), vm((2 * TOK, 512), BF16),
            vm((8, 2 * TOK, 256), BF16), vm((2, NY, TOK, 256), BF16), vm((NY, NX, TOK, 256), BF16),
            vm((2, TOK, 256), BF16), vm((NY, TOK, 256), BF16), vm((4, TOK, 256), BF16),
            dma((15,)), dma((NX,)), dma, dma((NX,)), dma, dma((NX,)), dma, dma((NZ,)), dma,
            dma((16,)), dma, dma((2, 4)), dma((2,)), dma((4, 2)), dma((4,)), dma((2,)), dma((4,)), dma, dma((16,)), dma, dma((2, 14)), dma((2, 14)),
            dma((30,)), dma((2,)), dma, dma,
        ],
        compiler_params=pltpu.CompilerParams(
            collective_id=0, has_side_effects=True, vmem_limit_bytes=60 * 1024 * 1024
        ),
        name="layer",
    )(
        residual, lifted, pace, fading, rate_l, rate_s, turn_l, turn_s,
        proj_l.swapaxes(-1, -2), proj_s.swapaxes(-1, -2),
        skip.reshape(8, CH), closing.reshape(8, CH), emitted, leading.reshape(1, D), raising, lowering.T,
    )


def solution(mesh):
    rest = [P()] * 10
    return jax.shard_map(
        on_device,
        mesh=mesh,
        in_specs=(P("sp", "tp"), P("sp", "tp"), P("tp", "sp"), P("tp", "sp"), *rest, P("sp", "tp"), P("tp", "sp")),
        out_specs=P("sp", "tp"),
        check_vma=False,
    )
```

```python
import jax
import jax.numpy as jnp
from jax import lax
from jax.experimental import pallas as pl
from jax.experimental.pallas import tpu as pltpu
from jax.sharding import PartitionSpec as P

F32 = jnp.float32
BF16 = jnp.bfloat16
HI = lax.Precision.HIGHEST
MESH = pl.DeviceIdType.MESH
EPSILON = 1e-6

NX, NY, NZ = 4, 4, 8
TOK = 128
CH = 128
ST = 384
LONG = 256
D = 2048
STEPS = 16
CHUNKS = 8


def iota(shape, dim):
    return lax.broadcasted_iota(jnp.int32, shape, dim)


def one_hot(pred):
    return jnp.where(pred, 1.0, 0.0).astype(F32)


def nt(a, b, precision=None):
    return lax.dot_general(
        a, b, (((1,), (1,)), ((), ())), precision=precision, preferred_element_type=F32
    )


def mm(a, b, precision=None):
    return jnp.dot(a, b, precision=precision, preferred_element_type=F32)


def halves(a):
    high = a.astype(BF16)
    return high, (a - high.astype(F32)).astype(BF16)


def sincos(a):
    k = jnp.floor(a * 0.6366197723675814 + 0.5)
    r = ((a - k * 1.5703125) - k * 4.837512969970703125e-4) - k * 7.549789948768648e-8
    z = r * r
    s = ((-1.9515295891e-4 * z + 8.3321608736e-3) * z - 1.6666654611e-1) * z * r + r
    c = ((2.443315711809948e-5 * z - 1.388731625493765e-3) * z + 4.166664568298827e-2) * z * z
    c = c - 0.5 * z + 1.0
    half = jnp.floor(k * 0.5)
    odd = (k - 2.0 * half) > 0.5
    low = half - 2.0 * jnp.floor(half * 0.5)
    sin_sign = 1.0 - 2.0 * low
    cos_sign = jnp.where(odd, -sin_sign, sin_sign)
    return jnp.where(odd, c, s) * sin_sign, jnp.where(odd, s, c) * cos_sign


def lost(u):
    poly = 1.0 - u * (1.0 / 8)
    for n in (7, 6, 5, 4, 3, 2):
        poly = 1.0 - u * poly * (1.0 / n)
    return jnp.where(u < 0.6, u * poly, 1.0 - jnp.exp(-u))


def kernel(
    residual, lifted, pace, fading, rate_l, rate_s, turn_l, turn_s, proj_l, proj_s,
    skip, closing, emitted, leading, raising, lowering,
    out,
    lifted_v, pace_v, fading_v, rate_lv, rate_sv, turn_lv, turn_sv, proj_lv, proj_sv,
    skip_v, closing_v, raising_v, lowering_v, emitted_v, leading_v,
    maps_v, pace_s, fading_s, drive_s, prefix_s, state_s, lifted_s,
    ends, cx, cz, row_ends, merged_v, gathered, res_v, mid_v, mid_f, own_mid,
    weights, hidden, partial, from_y, from_x, sum_y, sum_x, final,
    load_sem, up_send, up_recv, down_recv, cx_send, cx_recv, cz_send, cz_recv,
    mg_send, mg_recv, ay_send, ay_recv, ax_send, ax_recv, fy_send, fx_send, final_recv, res_send, res_recv, ring_send, ring_recv,
    sib_send, sib_recv, mid_send, mid_recv,
):
    sp = lax.axis_index("sp")
    tp = lax.axis_index("tp")
    z, x = sp // NX, sp % NX
    y, c = tp // 2, tp % 2
    sib = y * 2 + (1 - c)
    chip = x * NY + y
    block = x // 2
    inner = x % 2

    def remote(src, dst, send, recv, to):
        return pltpu.make_async_remote_copy(
            src_ref=src, dst_ref=dst, send_sem=send, recv_sem=recv,
            device_id=to, device_id_type=MESH,
        )

    def arrival(ref, sem):
        pltpu.make_async_copy(ref, ref, sem).wait()

    loads = [
        (lifted, lifted_v), (pace, pace_v), (fading, fading_v), (rate_l, rate_lv),
        (rate_s, rate_sv), (turn_l, turn_lv), (turn_s, turn_sv),
        (proj_l.at[:, :, :, pl.ds(tp * 4, 4)], proj_lv),
        (proj_s.at[:, :, :, pl.ds(tp * 4, 4)], proj_sv),
        (skip, skip_v), (closing, closing_v), (raising, raising_v), (lowering, lowering_v),
        (leading, leading_v), (emitted, emitted_v),
    ]
    copies = [pltpu.make_async_copy(a, b, load_sem.at[n]) for n, (a, b) in enumerate(loads)]
    for copy in copies:
        copy.start()

    barrier = pltpu.get_barrier_semaphore()
    spot = x * 8 + tp

    @pl.loop(1, 32)
    def _(off):
        to = (spot + off) % 32
        pl.semaphore_signal(barrier, inc=1, device_id=(z * NX + to // 8, to % 8), device_id_type=MESH)

    @pl.loop(1, NZ)
    def _(off):
        pl.semaphore_signal(
            barrier, inc=1, device_id=(((z + off) % NZ) * NX + x, tp), device_id_type=MESH
        )

    for copy in copies[:-4]:
        copy.wait()

    r2, t2 = iota((TOK, TOK), 0), iota((TOK, TOK), 1)
    perm = one_hot(t2 == (r2 & 7) * STEPS + (r2 >> 3))
    perm_back = one_hot(r2 == (t2 & 7) * STEPS + (t2 >> 3))
    p8, g8 = iota((8, ST), 1), iota((8, ST), 0)
    group8 = jnp.where(p8 < LONG, (p8 >> 6) * 2, ((p8 - LONG) >> 5) * 2 + 1)
    spread = one_hot(g8 == group8)
    pace_s[...] = mm(nt(perm, pace_v[...], HI), spread, HI)
    fading_s[...] = mm(nt(perm, fading_v[...], HI), spread, HI)
    lifted_p = mm(perm.astype(BF16), lifted_v[...])
    lifted_s[...] = lifted_p

    def flat(long_ref, short_ref, e):
        a = mm(long_ref[e], one_hot(iota((64, LONG), 0) == (iota((64, LONG), 1) & 63)), HI)
        own = iota((32, LONG), 0) == tp * 4 + (iota((32, LONG), 1) >> 6)
        a = jnp.sum(jnp.where(own, a, 0.0), axis=0, keepdims=True)
        b = mm(short_ref[e], one_hot(iota((32, CH), 0) == (iota((32, CH), 1) & 31)), HI)
        own = iota((32, CH), 0) == tp * 4 + (iota((32, CH), 1) >> 5)
        b = jnp.sum(jnp.where(own, b, 0.0), axis=0, keepdims=True)
        return jnp.concatenate([a, b], axis=1)

    rates = [flat(rate_lv, rate_sv, e) for e in range(2)]
    turns = [flat(turn_lv, turn_sv, e) for e in range(2)]

    tile_l = one_hot(iota((64, LONG), 0) == (iota((64, LONG), 1) & 63)).astype(BF16)
    tile_s = one_hot(iota((32, CH), 0) == (iota((32, CH), 1) & 31)).astype(BF16)
    own_l = (iota((64, LONG), 0) >> 4) == (iota((64, LONG), 1) >> 6)
    own_s = (iota((64, CH), 0) >> 4) == (iota((64, CH), 1) >> 5)
    maps_v[...] = jnp.zeros(maps_v.shape, BF16)
    for e in range(2):
        for io in range(2):
            for part in range(2):
                wide = halves(proj_lv[e, io, part].reshape(64, 64))
                slim = halves(proj_sv[e, io, part].reshape(64, 32))
                for h in range(2):
                    a = jnp.where(own_l, mm(wide[h], tile_l), 0.0).astype(BF16)
                    b = jnp.where(own_s, mm(slim[h], tile_s), 0.0).astype(BF16)
                    for n in range(4):
                        rows = slice(16 * n, 16 * n + 16)
                        maps_v[e, io, part, h, 32 * n : 32 * n + 16, :LONG] = a[rows]
                        maps_v[e, io, part, h, 32 * n + 16 : 32 * n + 32, LONG:] = b[rows]
    lifted_b = lifted_p.astype(BF16)
    for e in range(2):
        for part in range(2):
            drive_s[e, part] = mm(lifted_b, maps_v[e, 0, part, 0]) + mm(lifted_b, maps_v[e, 0, part, 1])

    def step(s, carry):
        new = []
        for e in range(2):
            rows = pl.ds(pl.multiple_of((s if e == 0 else STEPS - 1 - s) * 8, 8), 8)
            pre, pim, hre, him = carry[4 * e : 4 * e + 4]
            dt = pace_s[rows, :]
            fade = rates[e] * dt
            mag = jnp.exp(fading_s[rows, :] - fade)
            sn, cs = sincos(turns[e] * dt)
            are, aim = mag * cs, mag * sn
            gain = jnp.sqrt(lost(2.0 * fade))
            bre, bim = drive_s[e, 0, rows, :] * gain, drive_s[e, 1, rows, :] * gain
            pre, pim = are * pre - aim * pim, are * pim + aim * pre
            hre, him = are * hre - aim * him + bre, are * him + aim * hre + bim
            prefix_s[e, 0, rows, :] = pre
            prefix_s[e, 1, rows, :] = pim
            state_s[e, 0, rows, :] = hre
            state_s[e, 1, rows, :] = him
            new += [pre, pim, hre, him]
        return tuple(new)

    one, zero = jnp.ones((8, ST), F32), jnp.zeros((8, ST), F32)
    tops = lax.fori_loop(0, STEPS // 2, step, (one, zero, zero, zero) * 2)

    copies[-4].wait()
    copies[-3].wait()
    pl.semaphore_wait(barrier, 31 + NZ - 1)


    def begin(copy):
        copy.start()

    def pieces(off):
        xt = (x + off) % NX
        up_src = raising_v.at[:, pl.ds(pl.multiple_of(xt * 256, 256), 256)]
        up_dst = weights.at[0, z, c, pl.ds(x * 64, 64), :]
        down_src = lowering_v.at[:, pl.ds(pl.multiple_of(xt * 256, 256), 256)]
        down_dst = weights.at[1, z, c, pl.ds(x * 64, 64), :]
        return xt, up_src, up_dst, down_src, down_dst

    for off in (2, 1, 3):
        xt, src, dst, _, _ = pieces(off)
        begin(remote(src, dst, up_send, up_recv, (z * NX + xt, tp)))
    for off in (2, 1, 3):
        xt, _, _, src, dst = pieces(off)
        begin(remote(src, dst, up_send, down_recv, (z * NX + xt, tp)))
    _, up_src, up_dst, down_src, down_dst = pieces(0)
    pltpu.make_async_copy(up_src, up_dst, up_recv).start()
    pltpu.make_async_copy(down_src, down_dst, down_recv).start()

    tops = lax.fori_loop(STEPS // 2, STEPS, step, tops)

    def composed(first, later):
        fre, fim, bre, bim = first
        nre, nim, are, aim = later
        return (
            nre * fre - nim * fim, nre * fim + nim * fre,
            nre * bre - nim * bim + are, nre * bim + nim * bre + aim,
        )

    unit = (jnp.ones((1, ST), F32),) + (jnp.zeros((1, ST), F32),) * 3
    before = []
    totals = []
    for e in range(2):
        run, rows = unit, [None] * CHUNKS
        for n in range(CHUNKS):
            n = n if e == 0 else CHUNKS - 1 - n
            rows[n] = run
            run = composed(run, tuple(m[n : n + 1] for m in tops[4 * e : 4 * e + 4]))
        before.append(tuple(jnp.concatenate([r[q] for r in rows], axis=0) for q in range(4)))
        totals += list(run)
    own_ends = jnp.concatenate(totals, axis=0)
    ends[...] = own_ends
    cx[x] = own_ends

    for off in (2, 1, 3):
        copy = remote(ends, cx.at[x], cx_send, cx_recv, (z * NX + (x + off) % NX, tp))
        copy.start()
    ORDER = (
        (0, 0, 0), (0, 1, 0), (1, 0, 0), (0, 0, 1), (0, 1, 1), (1, 1, 0), (0, 0, 2),
        (0, 1, 2), (1, 0, 1), (0, 0, 3), (1, 1, 1), (1, 0, 2), (1, 1, 2), (1, 0, 3),
    )

    def piece(way, slot, extra):
        kind, half, hops = ORDER[slot]
        hops = hops + extra
        zs = (z + (NZ - hops if way == 0 else hops)) % NZ
        return kind, weights.at[kind, zs, c, pl.ds((half ^ way) * 128, 128), :]

    def share(kind, ref):
        begin(remote(ref, ref, sib_send, sib_recv.at[kind], (sp, sib)))

    def ring_send_slot(slot):
        for way in range(2):
            to = ((z + (1 if way == 0 else NZ - 1)) % NZ) * NX + x
            _, ref = piece(way, slot, 0)
            begin(remote(ref, ref, ring_send, ring_recv.at[way, slot], (to, tp)))

    def ring_take(slot):
        for way in range(2):
            kind, ref = piece(way, slot, 1)
            arrival(ref, ring_recv.at[way, slot])
            share(kind, ref)

    own_block = pl.ds(pl.multiple_of(inner * TOK, TOK), TOK)

    def plane(off):
        to = (chip + off) % (NX * NY)
        return (z * NX + to // NY, (to % NY) * 2 + block)

    def to_plane(src, dst, send, recv):
        @pl.loop(1, NX * NY)
        def _(off):
            remote(src, dst, send.at[0], recv, plane(off)).start()

        @pl.when(c == block)
        def _():
            pltpu.make_async_copy(src, dst, recv).start()

        @pl.when(c != block)
        def _():
            remote(src, dst, send.at[1], recv, plane(0)).start()

    def plane_sent(src, dst, send, recv, fifteen):
        arrival(fifteen, send.at[0])

        @pl.when(c != block)
        def _():
            remote(src, dst, send.at[1], recv, plane(0)).wait_send()

    res_dst = res_v.at[own_block, pl.ds(pl.multiple_of(tp * 256, 256), 256)]
    arrival(weights.at[0, z, c], up_recv)
    ring_send_slot(0)
    ring_send_slot(1)
    share(0, weights.at[0, z, c])
    to_plane(residual, res_dst, res_send, res_recv)

    arrival(cx.at[pl.ds(0, NX - 1)], cx_recv)

    def as_map(ref, n, top):
        return tuple(ref[n, top + q : top + q + 1, :] for q in range(4))

    row = []
    for e in range(2):
        run = unit
        for n in range(NX) if e == 0 else reversed(range(NX)):
            run = composed(run, as_map(cx, n, 4 * e))
        row += list(run)
    row_ends[0] = jnp.concatenate(row[:4], axis=0)
    row_ends[1] = jnp.concatenate(row[4:], axis=0)
    cz[z] = jnp.concatenate(row[:4], axis=0)
    for off in (4, 3, 5, 2, 6, 1, 7):
        copy = remote(
            row_ends.at[jnp.where(z + off < NZ, 0, 1)], cz.at[z], cz_send, cz_recv,
            (((z + off) % NZ) * NX + x, tp),
        )
        copy.start()

    arrival(weights.at[1, z, c], down_recv)
    ring_send_slot(2)
    share(1, weights.at[1, z, c])
    ring_take(0)
    ring_send_slot(3)
    ring_take(1)
    ring_send_slot(4)
    ring_send_slot(5)

    arrival(cz.at[pl.ds(0, NZ - 1)], cz_recv)

    def applied(m, state):
        pre, pim, hre, him = m
        re, im = state
        return pre * re - pim * im + hre, pre * im + pim * re + him

    blank = jnp.zeros((1, ST), F32)
    out_y = jnp.zeros((TOK, CH), F32)
    for e in range(2):
        state = (blank, blank)
        for ref, count, at, top in ((cz, NZ, z, 0), (cx, NX, x, 4 * e)):
            for n in range(count) if e == 0 else reversed(range(count)):
                passed = (n < at) if e == 0 else (n > at)
                new = applied(as_map(ref, n, top), state)
                state = tuple(jnp.where(passed, a, b) for a, b in zip(new, state))
        entry = applied(before[e], state)
        tall = tuple(jnp.concatenate([v] * STEPS, axis=0) for v in entry)
        pre, pim = prefix_s[e, 0], prefix_s[e, 1]
        re = state_s[e, 0] + pre * tall[0] - pim * tall[1]
        im = state_s[e, 1] + pre * tall[1] + pim * tall[0]
        for part, value in ((0, re), (1, -im)):
            high, low = halves(value)
            out_y = out_y + nt(high, maps_v[e, 1, part, 0])
            out_y = out_y + (nt(low, maps_v[e, 1, part, 0]) + nt(high, maps_v[e, 1, part, 1]))

    mine = iota((8, CH), 0) == tp
    skip_row = jnp.sum(jnp.where(mine, skip_v[...], 0.0), axis=0, keepdims=True)
    closing_row = jnp.sum(jnp.where(mine, closing_v[...], 0.0), axis=0, keepdims=True)
    v = out_y + skip_row * lifted_s[...]
    act = 0.5 * v * (1.0 + jnp.tanh(0.7978845608028654 * (v + 0.044715 * v * v * v)))
    act = act * lax.rsqrt(jnp.mean(act * act, axis=1, keepdims=True) + EPSILON) * closing_row
    merged_v[...] = mm(perm_back.astype(BF16), act.astype(BF16)).astype(BF16)
    mg_dst = gathered.at[own_block, pl.ds(pl.multiple_of(tp * CH, CH), CH)]
    to_plane(merged_v, mg_dst, mg_send, mg_recv)

    ring_take(2)
    ring_take(3)
    ring_send_slot(6)
    ring_take(4)
    ring_send_slot(7)
    ring_send_slot(8)
    ring_take(5)
    ring_take(6)
    ring_send_slot(9)
    ring_send_slot(10)
    ring_take(7)
    ring_take(8)
    ring_send_slot(11)
    ring_take(9)
    ring_take(10)
    ring_send_slot(12)
    ring_take(11)
    ring_send_slot(13)
    copies[-1].wait()
    copies[-2].wait()
    arrival(res_v, res_recv)
    arrival(gathered, mg_recv)

    def project(n, squares):
        cols = pl.ds(pl.multiple_of(n * 512, 512), 512)
        m = mm(gathered[...], emitted_v[:, cols]) + res_v[:, cols].astype(F32)
        mid_f[:, cols] = m
        mid_v[:, cols] = (m * leading_v[:, cols]).astype(BF16)
        return squares + jnp.sum(m * m, axis=1, keepdims=True)

    squares = lax.fori_loop(0, 2, project, jnp.zeros((2 * TOK, 1), F32))
    ring_take(12)
    squares = lax.fori_loop(2, 4, project, squares)
    scale = lax.rsqrt(squares * (1.0 / D) + EPSILON)

    own_cols = pl.ds(pl.multiple_of(tp * 256, 256), 256)
    sib_cols = pl.ds(pl.multiple_of(sib * 256, 256), 256)

    @pl.when(c == block)
    def _():
        remote(mid_f.at[own_block, sib_cols], own_mid, mid_send, mid_recv, (sp, sib)).start()

    arrival(weights.at[0, :, 1 - c], sib_recv.at[0])
    for n in range(2):
        up = mm(mid_v[...], weights[0, :, n].reshape(D, 256)) * scale
        up = jnp.maximum(up, 0.0)
        hidden[:, n * 256 : (n + 1) * 256] = (up * up).astype(BF16)
    ring_take(13)
    arrival(weights.at[1, :, 1 - c], sib_recv.at[1])

    def down(*ns):
        both = [nt(hidden[:, :256], weights[1, n, 0]) + nt(hidden[:, 256:], weights[1, n, 1]) for n in ns]
        for n, value in zip(ns, both):
            partial[n] = value.astype(BF16)

    def row_of(k):
        return (y + 1 + k) % NY

    def along_y(i, k):
        to = row_of(k)
        src = partial.at[2 * to + 1, pl.ds(i * TOK, TOK), :]
        dst = from_y.at[i, y]
        return src, dst, remote(src, dst, ay_send, ay_recv.at[i], (sp, 2 * to + c))

    def along_x(k, i):
        src = partial.at[2 * row_of(k), pl.ds(i * TOK, TOK), :]
        dst = from_x.at[row_of(k), x]
        to = (z * NX + 2 * c + i, tp)
        return src, dst, remote(src, dst, ax_send, ax_recv.at[k], to)

    def on_y(i):
        dst = final.at[x]
        to = (z * NX + 2 * c + i, y * 2 + 1)
        return sum_y.at[i], dst, remote(sum_y.at[i], dst, fy_send.at[i], final_recv, to)

    def on_x(k):
        dst = final.at[y]
        to = (sp, row_of(k) * 2)
        return sum_x.at[k], dst, remote(sum_x.at[k], dst, fx_send.at[k], final_recv, to)

    def deliver(triple, recv, local):
        src, dst, copy = triple
        if local is None:
            copy.start()
            return

        @pl.when(local)
        def _():
            pltpu.make_async_copy(src, dst, recv).start()

        @pl.when(jnp.logical_not(local))
        def _():
            copy.start()

    def delivered(triple, local):
        if local is None:
            triple[2].wait_send()
            return

        @pl.when(jnp.logical_not(local))
        def _():
            triple[2].wait_send()

    def near(i):
        return (2 * c + i) == x

    def local_y(k):
        return (c == 0) if k == NY - 1 else None

    for k in (0, 2, 1, 3):
        down(2 * row_of(k) + 1, 2 * row_of(k))
        if k < NY - 1:
            along_y(0, k)[2].start()
        else:
            for i in range(2):
                src, dst, _ = along_y(i, k)
                pltpu.make_async_copy(src, dst, ay_recv.at[i]).start()
        for i in range(2):
            deliver(along_x(k, i), ax_recv.at[k], near(i))
        if k == 2:
            for n in (0, 2):
                along_y(1, n)[2].start()
        if k == 1:
            along_y(1, k)[2].start()

    def summed(ref):
        total = ref[0].astype(F32)
        for n in range(1, NX):
            total = total + ref[n].astype(F32)
        return total

    def turn_x(k):
        @pl.when(c == block)
        def _():
            arrival(from_x.at[row_of(k)], ax_recv.at[k])
            sum_x[k] = summed(from_x.at[row_of(k)]).astype(BF16)
            deliver(on_x(k), final_recv, local_y(k))

    def turn_y(i):
        arrival(from_y.at[i], ay_recv.at[i])
        sum_y[i] = summed(from_y.at[i]).astype(BF16)
        deliver(on_y(i), final_recv, jnp.logical_and(near(i), c == 1))

    @pl.when(c == block)
    def _():
        own_mid_copy = pltpu.make_async_copy(mid_f.at[own_block, own_cols], own_mid, mid_recv)
        own_mid_copy.start()

    turn_x(0)
    turn_x(2)
    turn_y(0)
    turn_x(1)
    turn_x(3)
    turn_y(1)

    arrival(hidden.at[pl.ds(0, 192), :], up_send)
    arrival(cx.at[pl.ds(0, NX - 1)], cx_send)
    arrival(cz.at[pl.ds(0, NZ - 1)], cz_send)
    arrival(weights.at[0, pl.ds(0, 7)], ring_send)
    arrival(weights.at[0], sib_send)
    plane_sent(residual, res_dst, res_send, res_recv, res_v.at[pl.ds(0, 240), :])
    plane_sent(merged_v, mg_dst, mg_send, mg_recv, gathered.at[pl.ds(0, 240), :])

    @pl.when(c == block)
    def _():
        remote(mid_f.at[own_block, sib_cols], own_mid, mid_send, mid_recv, (sp, sib)).wait_send()

    arrival(own_mid, mid_recv)
    arrival(final, final_recv)
    out[...] = (own_mid[...] + summed(final)).astype(BF16)

    arrival(partial.at[pl.ds(0, 3)], ay_send)

    @pl.when(c == block)
    def _():
        arrival(partial.at[pl.ds(0, 2)], ax_send)
        for k in range(NY):
            delivered(on_x(k), local_y(k))

    @pl.when(c != block)
    def _():
        arrival(partial.at[pl.ds(0, 4)], ax_send)

    for i in range(2):
        delivered(on_y(i), jnp.logical_and(near(i), c == 1))


def on_device(
    residual, lifted, pace, fading, rate_l, rate_s, turn_l, turn_s, proj_l, proj_s,
    skip, closing, emitted, leading, raising, lowering,
):
    dma = pltpu.SemaphoreType.DMA
    vm = pltpu.VMEM
    return pl.pallas_call(
        kernel,
        out_shape=pltpu.VMEM((TOK, 256), BF16),
        in_specs=[pl.BlockSpec(memory_space=pl.ANY)] * 16,
        out_specs=pl.BlockSpec(memory_space=pltpu.VMEM),
        scratch_shapes=[
            vm((TOK, CH), BF16), vm((8, TOK), F32), vm((8, TOK), F32),
            vm((2, 32, 64), F32), vm((2, 32, 32), F32), vm((2, 32, 64), F32), vm((2, 32, 32), F32),
            vm((2, 2, 2, 4, 16, 64), F32), vm((2, 2, 2, 4, 16, 32), F32),
            vm((8, CH), F32), vm((8, CH), F32), vm((64, 1024), BF16), vm((64, 1024), BF16), vm((1024, D), BF16), vm((1, D), F32),
            vm((2, 2, 2, 2, CH, ST), BF16), vm((TOK, ST), F32), vm((TOK, ST), F32),
            vm((2, 2, TOK, ST), F32), vm((2, 2, TOK, ST), F32), vm((2, 2, TOK, ST), F32),
            vm((TOK, CH), F32),
            vm((8, ST), F32), vm((NX, 8, ST), F32), vm((NZ, 4, ST), F32), vm((2, 4, ST), F32),
            vm((TOK, CH), BF16), vm((2 * TOK, 1024), BF16), vm((2 * TOK, D), BF16),
            vm((2 * TOK, D), BF16), vm((2 * TOK, D), F32), vm((TOK, 256), F32),
            vm((2, NZ, 2, 256, 256), BF16), vm((2 * TOK, 512), BF16),
            vm((8, 2 * TOK, 256), BF16), vm((2, NY, TOK, 256), BF16), vm((NY, NX, TOK, 256), BF16),
            vm((2, TOK, 256), BF16), vm((NY, TOK, 256), BF16), vm((4, TOK, 256), BF16),
            dma((15,)), dma, dma, dma, dma, dma, dma, dma,
            dma((2,)), dma, dma, dma((2,)), dma, dma((4,)), dma((2,)), dma((4,)), dma,
            dma((2,)), dma, dma, dma((2, 14)), dma, dma((2,)), dma, dma,
        ],
        compiler_params=pltpu.CompilerParams(
            collective_id=0, has_side_effects=True, vmem_limit_bytes=60 * 1024 * 1024
        ),
        name="layer",
    )(
        residual, lifted, pace, fading, rate_l, rate_s, turn_l, turn_s,
        proj_l.swapaxes(-1, -2), proj_s.swapaxes(-1, -2),
        skip.reshape(8, CH), closing.reshape(8, CH), emitted, leading.reshape(1, D), raising, lowering.T,
    )


def solution(mesh):
    rest = [P()] * 10
    return jax.shard_map(
        on_device,
        mesh=mesh,
        in_specs=(P("sp", "tp"), P("sp", "tp"), P("tp", "sp"), P("tp", "sp"), *rest, P("sp", "tp"), P("tp", "sp")),
        out_specs=P("sp", "tp"),
        check_vma=False,
    )
```

```python
import jax
import jax.numpy as jnp
from jax import lax
from jax.experimental import pallas as pl
from jax.experimental.pallas import tpu as pltpu
from jax.sharding import PartitionSpec as P

F32 = jnp.float32
BF16 = jnp.bfloat16
HI = lax.Precision.HIGHEST
MESH = pl.DeviceIdType.MESH
EPSILON = 1e-6

NX, NY, NZ = 4, 4, 8
TOK = 128
CH = 128
ST = 384
LONG = 256
D = 2048
STEPS = 16
CHUNKS = 8


def iota(shape, dim):
    return lax.broadcasted_iota(jnp.int32, shape, dim)


def one_hot(pred):
    return jnp.where(pred, 1.0, 0.0).astype(F32)


def nt(a, b, precision=None):
    return lax.dot_general(
        a, b, (((1,), (1,)), ((), ())), precision=precision, preferred_element_type=F32
    )


def mm(a, b, precision=None):
    return jnp.dot(a, b, precision=precision, preferred_element_type=F32)


def halves(a):
    high = a.astype(BF16)
    return high, (a - high.astype(F32)).astype(BF16)


def sincos(a):
    k = jnp.floor(a * 0.6366197723675814 + 0.5)
    r = ((a - k * 1.5703125) - k * 4.837512969970703125e-4) - k * 7.549789948768648e-8
    z = r * r
    s = ((-1.9515295891e-4 * z + 8.3321608736e-3) * z - 1.6666654611e-1) * z * r + r
    c = ((2.443315711809948e-5 * z - 1.388731625493765e-3) * z + 4.166664568298827e-2) * z * z
    c = c - 0.5 * z + 1.0
    half = jnp.floor(k * 0.5)
    odd = (k - 2.0 * half) > 0.5
    low = half - 2.0 * jnp.floor(half * 0.5)
    sin_sign = 1.0 - 2.0 * low
    cos_sign = jnp.where(odd, -sin_sign, sin_sign)
    return jnp.where(odd, c, s) * sin_sign, jnp.where(odd, s, c) * cos_sign


def lost(u):
    poly = 1.0 - u * (1.0 / 8)
    for n in (7, 6, 5, 4, 3, 2):
        poly = 1.0 - u * poly * (1.0 / n)
    return jnp.where(u < 0.6, u * poly, 1.0 - jnp.exp(-u))


def kernel(
    residual, lifted, pace, fading, rate_l, rate_s, turn_l, turn_s, proj_l, proj_s,
    skip, closing, emitted, leading, raising, lowering,
    out,
    lifted_v, pace_v, fading_v, rate_lv, rate_sv, turn_lv, turn_sv, proj_lv, proj_sv,
    skip_v, closing_v, raising_v, lowering_v, emitted_v, leading_v,
    maps_v, pace_s, fading_s, drive_s, prefix_s, state_s, lifted_s,
    ends, cx, cz, row_ends, merged_v, gathered, res_v, mid_v, mid_f, own_mid,
    weights, hidden, partial, from_y, from_x, sum_y, sum_x, final,
    load_sem, up_send, up_recv, down_recv, cx_send, cx_recv, cz_send, cz_recv,
    mg_send, mg_recv, ay_send, ay_recv, ax_send, ax_recv, fy_send, fx_send, final_recv, res_send, res_recv, ring_send, ring_recv,
    sib_send, sib_recv, mid_send, mid_recv,
):
    sp = lax.axis_index("sp")
    tp = lax.axis_index("tp")
    z, x = sp // NX, sp % NX
    y, c = tp // 2, tp % 2
    sib = y * 2 + (1 - c)
    chip = x * NY + y
    block = x // 2
    inner = x % 2

    def remote(src, dst, send, recv, to):
        return pltpu.make_async_remote_copy(
            src_ref=src, dst_ref=dst, send_sem=send, recv_sem=recv,
            device_id=to, device_id_type=MESH,
        )

    def arrival(ref, sem):
        pltpu.make_async_copy(ref, ref, sem).wait()

    loads = [
        (lifted, lifted_v), (pace, pace_v), (fading, fading_v), (rate_l, rate_lv),
        (rate_s, rate_sv), (turn_l, turn_lv), (turn_s, turn_sv),
        (proj_l.at[:, :, :, pl.ds(tp * 4, 4)], proj_lv),
        (proj_s.at[:, :, :, pl.ds(tp * 4, 4)], proj_sv),
        (skip, skip_v), (closing, closing_v), (raising, raising_v), (lowering, lowering_v),
        (leading, leading_v), (emitted, emitted_v),
    ]
    copies = [pltpu.make_async_copy(a, b, load_sem.at[n]) for n, (a, b) in enumerate(loads)]
    for copy in copies:
        copy.start()

    barrier = pltpu.get_barrier_semaphore()
    spot = x * 8 + tp

    for off in (4, 3, 5, 2, 6, 1, 7):
        pl.semaphore_signal(
            barrier, inc=1, device_id=(((z + off) % NZ) * NX + x, tp), device_id_type=MESH
        )
    for off in sorted(range(1, 32), key=lambda n: abs(n - 16)):
        to = (spot + off) % 32
        pl.semaphore_signal(barrier, inc=1, device_id=(z * NX + to // 8, to % 8), device_id_type=MESH)

    for copy in copies[:-4]:
        copy.wait()

    r2, t2 = iota((TOK, TOK), 0), iota((TOK, TOK), 1)
    perm = one_hot(t2 == (r2 & 7) * STEPS + (r2 >> 3))
    perm_back = one_hot(r2 == (t2 & 7) * STEPS + (t2 >> 3))
    p8, g8 = iota((8, ST), 1), iota((8, ST), 0)
    group8 = jnp.where(p8 < LONG, (p8 >> 6) * 2, ((p8 - LONG) >> 5) * 2 + 1)
    spread = one_hot(g8 == group8)
    pace_s[...] = mm(nt(perm, pace_v[...], HI), spread, HI)
    fading_s[...] = mm(nt(perm, fading_v[...], HI), spread, HI)
    lifted_p = mm(perm.astype(BF16), lifted_v[...])
    lifted_s[...] = lifted_p

    def flat(long_ref, short_ref, e):
        a = mm(long_ref[e], one_hot(iota((64, LONG), 0) == (iota((64, LONG), 1) & 63)), HI)
        own = iota((32, LONG), 0) == tp * 4 + (iota((32, LONG), 1) >> 6)
        a = jnp.sum(jnp.where(own, a, 0.0), axis=0, keepdims=True)
        b = mm(short_ref[e], one_hot(iota((32, CH), 0) == (iota((32, CH), 1) & 31)), HI)
        own = iota((32, CH), 0) == tp * 4 + (iota((32, CH), 1) >> 5)
        b = jnp.sum(jnp.where(own, b, 0.0), axis=0, keepdims=True)
        return jnp.concatenate([a, b], axis=1)

    rates = [flat(rate_lv, rate_sv, e) for e in range(2)]
    turns = [flat(turn_lv, turn_sv, e) for e in range(2)]

    tile_l = one_hot(iota((64, LONG), 0) == (iota((64, LONG), 1) & 63)).astype(BF16)
    tile_s = one_hot(iota((32, CH), 0) == (iota((32, CH), 1) & 31)).astype(BF16)
    own_l = (iota((64, LONG), 0) >> 4) == (iota((64, LONG), 1) >> 6)
    own_s = (iota((64, CH), 0) >> 4) == (iota((64, CH), 1) >> 5)
    maps_v[...] = jnp.zeros(maps_v.shape, BF16)
    for e in range(2):
        for io in range(2):
            for part in range(2):
                wide = halves(proj_lv[e, io, part].reshape(64, 64))
                slim = halves(proj_sv[e, io, part].reshape(64, 32))
                for h in range(2):
                    a = jnp.where(own_l, mm(wide[h], tile_l), 0.0).astype(BF16)
                    b = jnp.where(own_s, mm(slim[h], tile_s), 0.0).astype(BF16)
                    for n in range(4):
                        rows = slice(16 * n, 16 * n + 16)
                        maps_v[e, io, part, h, 32 * n : 32 * n + 16, :LONG] = a[rows]
                        maps_v[e, io, part, h, 32 * n + 16 : 32 * n + 32, LONG:] = b[rows]
    lifted_b = lifted_p.astype(BF16)
    for e in range(2):
        for part in range(2):
            drive_s[e, part] = mm(lifted_b, maps_v[e, 0, part, 0]) + mm(lifted_b, maps_v[e, 0, part, 1])

    def step(s, carry):
        new = []
        for e in range(2):
            rows = pl.ds(pl.multiple_of((s if e == 0 else STEPS - 1 - s) * 8, 8), 8)
            pre, pim, hre, him = carry[4 * e : 4 * e + 4]
            dt = pace_s[rows, :]
            fade = rates[e] * dt
            mag = jnp.exp(fading_s[rows, :] - fade)
            sn, cs = sincos(turns[e] * dt)
            are, aim = mag * cs, mag * sn
            gain = jnp.sqrt(lost(2.0 * fade))
            bre, bim = drive_s[e, 0, rows, :] * gain, drive_s[e, 1, rows, :] * gain
            pre, pim = are * pre - aim * pim, are * pim + aim * pre
            hre, him = are * hre - aim * him + bre, are * him + aim * hre + bim
            prefix_s[e, 0, rows, :] = pre
            prefix_s[e, 1, rows, :] = pim
            state_s[e, 0, rows, :] = hre
            state_s[e, 1, rows, :] = him
            new += [pre, pim, hre, him]
        return tuple(new)

    one, zero = jnp.ones((8, ST), F32), jnp.zeros((8, ST), F32)
    tops = lax.fori_loop(0, STEPS // 2, step, (one, zero, zero, zero) * 2)

    copies[-4].wait()
    copies[-3].wait()
    pl.semaphore_wait(barrier, 31 + NZ - 1)


    def begin(copy):
        copy.start()

    def pieces(off):
        xt = (x + off) % NX
        up_src = raising_v.at[:, pl.ds(pl.multiple_of(xt * 256, 256), 256)]
        up_dst = weights.at[0, z, c, pl.ds(x * 64, 64), :]
        down_src = lowering_v.at[:, pl.ds(pl.multiple_of(xt * 256, 256), 256)]
        down_dst = weights.at[1, z, c, pl.ds(x * 64, 64), :]
        return xt, up_src, up_dst, down_src, down_dst

    for off in (2, 1, 3):
        xt, src, dst, _, _ = pieces(off)
        begin(remote(src, dst, up_send, up_recv, (z * NX + xt, tp)))
    _, up_src, up_dst, down_src, down_dst = pieces(0)
    pltpu.make_async_copy(up_src, up_dst, up_recv).start()


    tops = lax.fori_loop(STEPS // 2, STEPS, step, tops)

    def composed(first, later):
        fre, fim, bre, bim = first
        nre, nim, are, aim = later
        return (
            nre * fre - nim * fim, nre * fim + nim * fre,
            nre * bre - nim * bim + are, nre * bim + nim * bre + aim,
        )

    unit = (jnp.ones((1, ST), F32),) + (jnp.zeros((1, ST), F32),) * 3
    before = []
    totals = []
    for e in range(2):
        run, rows = unit, [None] * CHUNKS
        for n in range(CHUNKS):
            n = n if e == 0 else CHUNKS - 1 - n
            rows[n] = run
            run = composed(run, tuple(m[n : n + 1] for m in tops[4 * e : 4 * e + 4]))
        before.append(tuple(jnp.concatenate([r[q] for r in rows], axis=0) for q in range(4)))
        totals += list(run)
    own_ends = jnp.concatenate(totals, axis=0)
    ends[...] = own_ends
    cx[x] = own_ends

    for off in (2, 1, 3):
        copy = remote(ends, cx.at[x], cx_send, cx_recv, (z * NX + (x + off) % NX, tp))
        copy.start()
    for off in (2, 1, 3):
        xt, _, _, src, dst = pieces(off)
        begin(remote(src, dst, up_send, down_recv, (z * NX + xt, tp)))
    pltpu.make_async_copy(down_src, down_dst, down_recv).start()

    ORDER = (
        (0, 0, 0), (0, 1, 0), (1, 0, 0), (1, 1, 0), (0, 0, 1), (0, 1, 1), (1, 0, 1),
        (1, 1, 1), (0, 0, 2), (0, 1, 2), (1, 0, 2), (1, 1, 2), (0, 0, 3), (1, 0, 3),
    )

    def piece(way, slot, extra):
        kind, half, hops = ORDER[slot]
        hops = hops + extra
        zs = (z + (NZ - hops if way == 0 else hops)) % NZ
        return kind, weights.at[kind, zs, c, pl.ds((half ^ way) * 128, 128), :]

    def share(kind, ref):
        begin(remote(ref, ref, sib_send, sib_recv.at[kind], (sp, sib)))

    def ring_send_slot(slot):
        for way in range(2):
            to = ((z + (1 if way == 0 else NZ - 1)) % NZ) * NX + x
            _, ref = piece(way, slot, 0)
            begin(remote(ref, ref, ring_send, ring_recv.at[way, slot], (to, tp)))

    def ring_take(slot):
        for way in range(2):
            kind, ref = piece(way, slot, 1)
            arrival(ref, ring_recv.at[way, slot])
            share(kind, ref)

    own_block = pl.ds(pl.multiple_of(inner * TOK, TOK), TOK)

    def plane(off):
        to = (chip + off) % (NX * NY)
        return (z * NX + to // NY, (to % NY) * 2 + block)

    def to_plane(src, dst, send, recv):
        @pl.loop(1, NX * NY)
        def _(off):
            remote(src, dst, send.at[0], recv, plane(off)).start()

        @pl.when(c == block)
        def _():
            pltpu.make_async_copy(src, dst, recv).start()

        @pl.when(c != block)
        def _():
            remote(src, dst, send.at[1], recv, plane(0)).start()

    def plane_sent(src, dst, send, recv, fifteen):
        arrival(fifteen, send.at[0])

        @pl.when(c != block)
        def _():
            remote(src, dst, send.at[1], recv, plane(0)).wait_send()

    res_dst = res_v.at[own_block, pl.ds(pl.multiple_of(tp * 256, 256), 256)]
    arrival(weights.at[0, z, c], up_recv)
    ring_send_slot(0)
    share(0, weights.at[0, z, c])
    to_plane(residual, res_dst, res_send, res_recv)

    arrival(cx.at[pl.ds(0, NX - 1)], cx_recv)

    def as_map(ref, n, top):
        return tuple(ref[n, top + q : top + q + 1, :] for q in range(4))

    row = []
    for e in range(2):
        run = unit
        for n in range(NX) if e == 0 else reversed(range(NX)):
            run = composed(run, as_map(cx, n, 4 * e))
        row += list(run)
    row_ends[0] = jnp.concatenate(row[:4], axis=0)
    row_ends[1] = jnp.concatenate(row[4:], axis=0)
    cz[z] = jnp.concatenate(row[:4], axis=0)
    for off in (4, 3, 5, 2, 6, 1, 7):
        copy = remote(
            row_ends.at[jnp.where(z + off < NZ, 0, 1)], cz.at[z], cz_send, cz_recv,
            (((z + off) % NZ) * NX + x, tp),
        )
        copy.start()

    ring_send_slot(1)
    arrival(weights.at[1, z, c], down_recv)
    ring_send_slot(2)
    ring_send_slot(3)
    share(1, weights.at[1, z, c])
    ring_take(0)
    ring_send_slot(4)
    ring_take(1)
    ring_send_slot(5)

    arrival(cz.at[pl.ds(0, NZ - 1)], cz_recv)
    ring_take(2)
    ring_send_slot(6)

    def applied(m, state):
        pre, pim, hre, him = m
        re, im = state
        return pre * re - pim * im + hre, pre * im + pim * re + him

    blank = jnp.zeros((1, ST), F32)
    out_y = jnp.zeros((TOK, CH), F32)
    for e in range(2):
        state = (blank, blank)
        for ref, count, at, top in ((cz, NZ, z, 0), (cx, NX, x, 4 * e)):
            for n in range(count) if e == 0 else reversed(range(count)):
                passed = (n < at) if e == 0 else (n > at)
                new = applied(as_map(ref, n, top), state)
                state = tuple(jnp.where(passed, a, b) for a, b in zip(new, state))
        entry = applied(before[e], state)
        tall = tuple(jnp.concatenate([v] * STEPS, axis=0) for v in entry)
        pre, pim = prefix_s[e, 0], prefix_s[e, 1]
        re = state_s[e, 0] + pre * tall[0] - pim * tall[1]
        im = state_s[e, 1] + pre * tall[1] + pim * tall[0]
        for part, value in ((0, re), (1, -im)):
            high, low = halves(value)
            out_y = out_y + nt(high, maps_v[e, 1, part, 0])
            out_y = out_y + (nt(low, maps_v[e, 1, part, 0]) + nt(high, maps_v[e, 1, part, 1]))

    mine = iota((8, CH), 0) == tp
    skip_row = jnp.sum(jnp.where(mine, skip_v[...], 0.0), axis=0, keepdims=True)
    closing_row = jnp.sum(jnp.where(mine, closing_v[...], 0.0), axis=0, keepdims=True)
    v = out_y + skip_row * lifted_s[...]
    act = 0.5 * v * (1.0 + jnp.tanh(0.7978845608028654 * (v + 0.044715 * v * v * v)))
    act = act * lax.rsqrt(jnp.mean(act * act, axis=1, keepdims=True) + EPSILON) * closing_row
    merged_v[...] = mm(perm_back.astype(BF16), act.astype(BF16)).astype(BF16)
    mg_dst = gathered.at[own_block, pl.ds(pl.multiple_of(tp * CH, CH), CH)]
    to_plane(merged_v, mg_dst, mg_send, mg_recv)

    ring_take(3)
    ring_send_slot(7)
    ring_take(4)
    ring_send_slot(8)
    ring_take(5)
    ring_send_slot(9)
    ring_take(6)
    ring_send_slot(10)
    ring_take(7)
    ring_send_slot(11)
    ring_take(8)
    ring_send_slot(12)
    ring_take(9)
    ring_take(10)
    ring_send_slot(13)
    ring_take(11)
    copies[-1].wait()
    copies[-2].wait()
    arrival(res_v, res_recv)
    arrival(gathered, mg_recv)

    def project(n, squares):
        cols = pl.ds(n * 1024, 1024)
        m = mm(gathered[...], emitted_v[:, cols]) + res_v[:, cols].astype(F32)
        mid_f[:, cols] = m
        mid_v[:, cols] = (m * leading_v[:, cols]).astype(BF16)
        return squares + jnp.sum(m * m, axis=1, keepdims=True)

    squares = project(0, jnp.zeros((2 * TOK, 1), F32))
    ring_take(12)
    squares = project(1, squares)
    scale = lax.rsqrt(squares * (1.0 / D) + EPSILON)

    own_cols = pl.ds(pl.multiple_of(tp * 256, 256), 256)
    sib_cols = pl.ds(pl.multiple_of(sib * 256, 256), 256)

    @pl.when(c == block)
    def _():
        remote(mid_f.at[own_block, sib_cols], own_mid, mid_send, mid_recv, (sp, sib)).start()

    ring_take(13)
    arrival(weights.at[0, :, 1 - c], sib_recv.at[0])
    for n in range(2):
        up = mm(mid_v[...], weights[0, :, n].reshape(D, 256)) * scale
        up = jnp.maximum(up, 0.0)
        hidden[:, n * 256 : (n + 1) * 256] = (up * up).astype(BF16)
    arrival(weights.at[1, :, 1 - c], sib_recv.at[1])

    def down(*ns):
        both = [nt(hidden[:, :256], weights[1, n, 0]) + nt(hidden[:, 256:], weights[1, n, 1]) for n in ns]
        for n, value in zip(ns, both):
            partial[n] = value.astype(BF16)

    def row_of(k):
        return (y + 1 + k) % NY

    def along_y(i, k):
        to = row_of(k)
        src = partial.at[2 * to + 1, pl.ds(i * TOK, TOK), :]
        dst = from_y.at[i, y]
        return src, dst, remote(src, dst, ay_send, ay_recv.at[i], (sp, 2 * to + c))

    def along_x(k, i):
        src = partial.at[2 * row_of(k), pl.ds(i * TOK, TOK), :]
        dst = from_x.at[row_of(k), x]
        to = (z * NX + 2 * c + i, tp)
        return src, dst, remote(src, dst, ax_send, ax_recv.at[k], to)

    def on_y(i):
        dst = final.at[x]
        to = (z * NX + 2 * c + i, y * 2 + 1)
        return sum_y.at[i], dst, remote(sum_y.at[i], dst, fy_send.at[i], final_recv, to)

    def on_x(k):
        dst = final.at[y]
        to = (sp, row_of(k) * 2)
        return sum_x.at[k], dst, remote(sum_x.at[k], dst, fx_send.at[k], final_recv, to)

    def deliver(triple, recv, local):
        src, dst, copy = triple
        if local is None:
            copy.start()
            return

        @pl.when(local)
        def _():
            pltpu.make_async_copy(src, dst, recv).start()

        @pl.when(jnp.logical_not(local))
        def _():
            copy.start()

    def delivered(triple, local):
        if local is None:
            triple[2].wait_send()
            return

        @pl.when(jnp.logical_not(local))
        def _():
            triple[2].wait_send()

    def near(i):
        return (2 * c + i) == x

    def local_y(k):
        return (c == 0) if k == NY - 1 else None

    for k in (1, 0, 2, 3):
        down(2 * row_of(k) + 1, 2 * row_of(k))
        if k < NY - 1:
            along_y(0, k)[2].start()
        else:
            for i in range(2):
                src, dst, _ = along_y(i, k)
                pltpu.make_async_copy(src, dst, ay_recv.at[i]).start()
        for i in range(2):
            deliver(along_x(k, i), ax_recv.at[k], near(i))
        if k == 2:
            for n in (1, 0, 2):
                along_y(1, n)[2].start()

    def summed(ref):
        total = ref[0].astype(F32)
        for n in range(1, NX):
            total = total + ref[n].astype(F32)
        return total

    def turn_x(k):
        @pl.when(c == block)
        def _():
            arrival(from_x.at[row_of(k)], ax_recv.at[k])
            sum_x[k] = summed(from_x.at[row_of(k)]).astype(BF16)
            deliver(on_x(k), final_recv, local_y(k))

    def turn_y(i):
        arrival(from_y.at[i], ay_recv.at[i])
        sum_y[i] = summed(from_y.at[i]).astype(BF16)
        deliver(on_y(i), final_recv, jnp.logical_and(near(i), c == 1))

    @pl.when(c == block)
    def _():
        own_mid_copy = pltpu.make_async_copy(mid_f.at[own_block, own_cols], own_mid, mid_recv)
        own_mid_copy.start()

    turn_x(1)
    turn_x(0)
    turn_x(2)
    turn_x(3)
    turn_y(0)
    turn_y(1)

    arrival(hidden.at[pl.ds(0, 192), :], up_send)
    arrival(cx.at[pl.ds(0, NX - 1)], cx_send)
    arrival(cz.at[pl.ds(0, NZ - 1)], cz_send)
    arrival(weights.at[0, pl.ds(0, 7)], ring_send)
    arrival(weights.at[0], sib_send)
    plane_sent(residual, res_dst, res_send, res_recv, res_v.at[pl.ds(0, 240), :])
    plane_sent(merged_v, mg_dst, mg_send, mg_recv, gathered.at[pl.ds(0, 240), :])

    @pl.when(c == block)
    def _():
        remote(mid_f.at[own_block, sib_cols], own_mid, mid_send, mid_recv, (sp, sib)).wait_send()

    arrival(own_mid, mid_recv)
    arrival(final, final_recv)
    out[...] = (own_mid[...] + summed(final)).astype(BF16)

    arrival(partial.at[pl.ds(0, 3)], ay_send)

    @pl.when(c == block)
    def _():
        arrival(partial.at[pl.ds(0, 2)], ax_send)
        for k in range(NY):
            delivered(on_x(k), local_y(k))

    @pl.when(c != block)
    def _():
        arrival(partial.at[pl.ds(0, 4)], ax_send)

    for i in range(2):
        delivered(on_y(i), jnp.logical_and(near(i), c == 1))


def on_device(
    residual, lifted, pace, fading, rate_l, rate_s, turn_l, turn_s, proj_l, proj_s,
    skip, closing, emitted, leading, raising, lowering,
):
    dma = pltpu.SemaphoreType.DMA
    vm = pltpu.VMEM
    return pl.pallas_call(
        kernel,
        out_shape=pltpu.VMEM((TOK, 256), BF16),
        in_specs=[pl.BlockSpec(memory_space=pl.ANY)] * 16,
        out_specs=pl.BlockSpec(memory_space=pltpu.VMEM),
        scratch_shapes=[
            vm((TOK, CH), BF16), vm((8, TOK), F32), vm((8, TOK), F32),
            vm((2, 32, 64), F32), vm((2, 32, 32), F32), vm((2, 32, 64), F32), vm((2, 32, 32), F32),
            vm((2, 2, 2, 4, 16, 64), F32), vm((2, 2, 2, 4, 16, 32), F32),
            vm((8, CH), F32), vm((8, CH), F32), vm((64, 1024), BF16), vm((64, 1024), BF16), vm((1024, D), BF16), vm((1, D), F32),
            vm((2, 2, 2, 2, CH, ST), BF16), vm((TOK, ST), F32), vm((TOK, ST), F32),
            vm((2, 2, TOK, ST), F32), vm((2, 2, TOK, ST), F32), vm((2, 2, TOK, ST), F32),
            vm((TOK, CH), F32),
            vm((8, ST), F32), vm((NX, 8, ST), F32), vm((NZ, 4, ST), F32), vm((2, 4, ST), F32),
            vm((TOK, CH), BF16), vm((2 * TOK, 1024), BF16), vm((2 * TOK, D), BF16),
            vm((2 * TOK, D), BF16), vm((2 * TOK, D), F32), vm((TOK, 256), F32),
            vm((2, NZ, 2, 256, 256), BF16), vm((2 * TOK, 512), BF16),
            vm((8, 2 * TOK, 256), BF16), vm((2, NY, TOK, 256), BF16), vm((NY, NX, TOK, 256), BF16),
            vm((2, TOK, 256), BF16), vm((NY, TOK, 256), BF16), vm((4, TOK, 256), BF16),
            dma((15,)), dma, dma, dma, dma, dma, dma, dma,
            dma((2,)), dma, dma, dma((2,)), dma, dma((4,)), dma((2,)), dma((4,)), dma,
            dma((2,)), dma, dma, dma((2, 14)), dma, dma((2,)), dma, dma,
        ],
        compiler_params=pltpu.CompilerParams(
            collective_id=0, has_side_effects=True, vmem_limit_bytes=60 * 1024 * 1024
        ),
        name="layer",
    )(
        residual, lifted, pace, fading, rate_l, rate_s, turn_l, turn_s,
        proj_l.swapaxes(-1, -2), proj_s.swapaxes(-1, -2),
        skip.reshape(8, CH), closing.reshape(8, CH), emitted, leading.reshape(1, D), raising, lowering.T,
    )


def solution(mesh):
    rest = [P()] * 10
    return jax.shard_map(
        on_device,
        mesh=mesh,
        in_specs=(P("sp", "tp"), P("sp", "tp"), P("tp", "sp"), P("tp", "sp"), *rest, P("sp", "tp"), P("tp", "sp")),
        out_specs=P("sp", "tp"),
        check_vma=False,
    )
```

```python
import jax
import jax.numpy as jnp
from jax import lax
from jax.experimental import pallas as pl
from jax.experimental.pallas import tpu as pltpu
from jax.sharding import PartitionSpec as P

F32 = jnp.float32
BF16 = jnp.bfloat16
HI = lax.Precision.HIGHEST
MESH = pl.DeviceIdType.MESH
EPSILON = 1e-6

NX, NY, NZ = 4, 4, 8
TOK = 128
CH = 128
ST = 384
LONG = 256
D = 2048
STEPS = 16
CHUNKS = 8


def iota(shape, dim):
    return lax.broadcasted_iota(jnp.int32, shape, dim)


def one_hot(pred):
    return jnp.where(pred, 1.0, 0.0).astype(F32)


def nt(a, b, precision=None):
    return lax.dot_general(
        a, b, (((1,), (1,)), ((), ())), precision=precision, preferred_element_type=F32
    )


def mm(a, b, precision=None):
    return jnp.dot(a, b, precision=precision, preferred_element_type=F32)


def halves(a):
    high = a.astype(BF16)
    return high, (a - high.astype(F32)).astype(BF16)


def sincos(a):
    k = jnp.floor(a * 0.6366197723675814 + 0.5)
    r = ((a - k * 1.5703125) - k * 4.837512969970703125e-4) - k * 7.549789948768648e-8
    z = r * r
    s = ((-1.9515295891e-4 * z + 8.3321608736e-3) * z - 1.6666654611e-1) * z * r + r
    c = ((2.443315711809948e-5 * z - 1.388731625493765e-3) * z + 4.166664568298827e-2) * z * z
    c = c - 0.5 * z + 1.0
    half = jnp.floor(k * 0.5)
    odd = (k - 2.0 * half) > 0.5
    low = half - 2.0 * jnp.floor(half * 0.5)
    sin_sign = 1.0 - 2.0 * low
    cos_sign = jnp.where(odd, -sin_sign, sin_sign)
    return jnp.where(odd, c, s) * sin_sign, jnp.where(odd, s, c) * cos_sign


def lost(u):
    poly = 1.0 - u * (1.0 / 8)
    for n in (7, 6, 5, 4, 3, 2):
        poly = 1.0 - u * poly * (1.0 / n)
    return jnp.where(u < 0.6, u * poly, 1.0 - jnp.exp(-u))


def kernel(
    residual, lifted, pace, fading, rate_l, rate_s, turn_l, turn_s, proj_l, proj_s,
    skip, closing, emitted, leading, raising, lowering,
    out,
    lifted_v, pace_v, fading_v, rate_lv, rate_sv, turn_lv, turn_sv, proj_lv, proj_sv,
    skip_v, closing_v, raising_v, lowering_v, emitted_v, leading_v,
    maps_v, pace_s, fading_s, drive_s, prefix_s, state_s, lifted_s,
    ends, cx, cz, row_ends, merged_v, gathered, res_v, mid_v, mid_f, own_mid,
    weights, hidden, partial, from_y, from_x, sum_y, sum_x, final,
    load_sem, up_send, up_recv, down_recv, cx_send, cx_recv, cz_send, cz_recv,
    mg_send, mg_recv, ay_send, ay_recv, ax_send, ax_recv, fy_send, fx_send, final_recv, res_send, res_recv, ring_send, ring_recv,
    sib_send, sib_recv, mid_send, mid_recv,
):
    sp = lax.axis_index("sp")
    tp = lax.axis_index("tp")
    z, x = sp // NX, sp % NX
    y, c = tp // 2, tp % 2
    sib = y * 2 + (1 - c)
    chip = x * NY + y
    block = x // 2
    inner = x % 2

    def remote(src, dst, send, recv, to):
        return pltpu.make_async_remote_copy(
            src_ref=src, dst_ref=dst, send_sem=send, recv_sem=recv,
            device_id=to, device_id_type=MESH,
        )

    def arrival(ref, sem):
        pltpu.make_async_copy(ref, ref, sem).wait()

    loads = [
        (lifted, lifted_v), (pace, pace_v), (fading, fading_v), (rate_l, rate_lv),
        (rate_s, rate_sv), (turn_l, turn_lv), (turn_s, turn_sv),
        (proj_l.at[:, :, :, pl.ds(tp * 4, 4)], proj_lv),
        (proj_s.at[:, :, :, pl.ds(tp * 4, 4)], proj_sv),
        (skip, skip_v), (closing, closing_v), (raising, raising_v), (lowering, lowering_v),
        (leading, leading_v), (emitted, emitted_v),
    ]
    copies = [pltpu.make_async_copy(a, b, load_sem.at[n]) for n, (a, b) in enumerate(loads)]
    for copy in copies:
        copy.start()

    barrier = pltpu.get_barrier_semaphore()
    spot = x * 8 + tp

    for off in (4, 3, 5, 2, 6, 1, 7):
        pl.semaphore_signal(
            barrier, inc=1, device_id=(((z + off) % NZ) * NX + x, tp), device_id_type=MESH
        )
    for off in sorted(range(1, 32), key=lambda n: abs(n - 16)):
        to = (spot + off) % 32
        pl.semaphore_signal(barrier, inc=1, device_id=(z * NX + to // 8, to % 8), device_id_type=MESH)

    for copy in copies[:-4]:
        copy.wait()

    r2, t2 = iota((TOK, TOK), 0), iota((TOK, TOK), 1)
    perm = one_hot(t2 == (r2 & 7) * STEPS + (r2 >> 3))
    perm_back = one_hot(r2 == (t2 & 7) * STEPS + (t2 >> 3))
    p8, g8 = iota((8, ST), 1), iota((8, ST), 0)
    group8 = jnp.where(p8 < LONG, (p8 >> 6) * 2, ((p8 - LONG) >> 5) * 2 + 1)
    spread = one_hot(g8 == group8)
    pace_s[...] = mm(nt(perm, pace_v[...], HI), spread, HI)
    fading_s[...] = mm(nt(perm, fading_v[...], HI), spread, HI)
    lifted_p = mm(perm.astype(BF16), lifted_v[...])
    lifted_s[...] = lifted_p

    def flat(long_ref, short_ref, e):
        a = mm(long_ref[e], one_hot(iota((64, LONG), 0) == (iota((64, LONG), 1) & 63)), HI)
        own = iota((32, LONG), 0) == tp * 4 + (iota((32, LONG), 1) >> 6)
        a = jnp.sum(jnp.where(own, a, 0.0), axis=0, keepdims=True)
        b = mm(short_ref[e], one_hot(iota((32, CH), 0) == (iota((32, CH), 1) & 31)), HI)
        own = iota((32, CH), 0) == tp * 4 + (iota((32, CH), 1) >> 5)
        b = jnp.sum(jnp.where(own, b, 0.0), axis=0, keepdims=True)
        return jnp.concatenate([a, b], axis=1)

    rates = [flat(rate_lv, rate_sv, e) for e in range(2)]
    turns = [flat(turn_lv, turn_sv, e) for e in range(2)]

    tile_l = one_hot(iota((64, LONG), 0) == (iota((64, LONG), 1) & 63)).astype(BF16)
    tile_s = one_hot(iota((32, CH), 0) == (iota((32, CH), 1) & 31)).astype(BF16)
    own_l = (iota((64, LONG), 0) >> 4) == (iota((64, LONG), 1) >> 6)
    own_s = (iota((64, CH), 0) >> 4) == (iota((64, CH), 1) >> 5)

    def build_maps(io):
        maps_v[:, io] = jnp.zeros((2, 2, 2, CH, ST), BF16)
        for e in range(2):
            for part in range(2):
                wide = halves(proj_lv[e, io, part].reshape(64, 64))
                slim = halves(proj_sv[e, io, part].reshape(64, 32))
                for h in range(2):
                    a = jnp.where(own_l, mm(wide[h], tile_l), 0.0).astype(BF16)
                    b = jnp.where(own_s, mm(slim[h], tile_s), 0.0).astype(BF16)
                    for n in range(4):
                        rows = slice(16 * n, 16 * n + 16)
                        maps_v[e, io, part, h, 32 * n : 32 * n + 16, :LONG] = a[rows]
                        maps_v[e, io, part, h, 32 * n + 16 : 32 * n + 32, LONG:] = b[rows]

    build_maps(0)
    lifted_b = lifted_p.astype(BF16)
    for e in range(2):
        for part in range(2):
            drive_s[e, part] = mm(lifted_b, maps_v[e, 0, part, 0]) + mm(lifted_b, maps_v[e, 0, part, 1])

    def step(s, carry):
        new = []
        for e in range(2):
            rows = pl.ds(pl.multiple_of((s if e == 0 else STEPS - 1 - s) * 8, 8), 8)
            pre, pim, hre, him = carry[4 * e : 4 * e + 4]
            dt = pace_s[rows, :]
            fade = rates[e] * dt
            mag = jnp.exp(fading_s[rows, :] - fade)
            sn, cs = sincos(turns[e] * dt)
            are, aim = mag * cs, mag * sn
            gain = jnp.sqrt(lost(2.0 * fade))
            bre, bim = drive_s[e, 0, rows, :] * gain, drive_s[e, 1, rows, :] * gain
            pre, pim = are * pre - aim * pim, are * pim + aim * pre
            hre, him = are * hre - aim * him + bre, are * him + aim * hre + bim
            prefix_s[e, 0, rows, :] = pre
            prefix_s[e, 1, rows, :] = pim
            state_s[e, 0, rows, :] = hre
            state_s[e, 1, rows, :] = him
            new += [pre, pim, hre, him]
        return tuple(new)

    one, zero = jnp.ones((8, ST), F32), jnp.zeros((8, ST), F32)
    tops = lax.fori_loop(0, STEPS // 4, step, (one, zero, zero, zero) * 2)

    copies[-4].wait()
    copies[-3].wait()
    pl.semaphore_wait(barrier, 31 + NZ - 1)


    def begin(copy):
        copy.start()

    def pieces(off):
        xt = (x + off) % NX
        up_src = raising_v.at[:, pl.ds(pl.multiple_of(xt * 256, 256), 256)]
        up_dst = weights.at[0, z, c, pl.ds(x * 64, 64), :]
        down_src = lowering_v.at[:, pl.ds(pl.multiple_of(xt * 256, 256), 256)]
        down_dst = weights.at[1, z, c, pl.ds(x * 64, 64), :]
        return xt, up_src, up_dst, down_src, down_dst

    for off in (2, 1, 3):
        xt, src, dst, _, _ = pieces(off)
        begin(remote(src, dst, up_send, up_recv, (z * NX + xt, tp)))
    _, up_src, up_dst, down_src, down_dst = pieces(0)
    pltpu.make_async_copy(up_src, up_dst, up_recv).start()


    tops = lax.fori_loop(STEPS // 4, STEPS, step, tops)

    def composed(first, later):
        fre, fim, bre, bim = first
        nre, nim, are, aim = later
        return (
            nre * fre - nim * fim, nre * fim + nim * fre,
            nre * bre - nim * bim + are, nre * bim + nim * bre + aim,
        )

    unit = (jnp.ones((1, ST), F32),) + (jnp.zeros((1, ST), F32),) * 3
    before = []
    totals = []
    for e in range(2):
        run, rows = unit, [None] * CHUNKS
        for n in range(CHUNKS):
            n = n if e == 0 else CHUNKS - 1 - n
            rows[n] = run
            run = composed(run, tuple(m[n : n + 1] for m in tops[4 * e : 4 * e + 4]))
        before.append(tuple(jnp.concatenate([r[q] for r in rows], axis=0) for q in range(4)))
        totals += list(run)
    own_ends = jnp.concatenate(totals, axis=0)
    ends[...] = own_ends
    cx[x] = own_ends

    for off in (2, 1, 3):
        copy = remote(ends, cx.at[x], cx_send, cx_recv, (z * NX + (x + off) % NX, tp))
        copy.start()
    for off in (2, 1, 3):
        xt, _, _, src, dst = pieces(off)
        begin(remote(src, dst, up_send, down_recv, (z * NX + xt, tp)))
    pltpu.make_async_copy(down_src, down_dst, down_recv).start()

    ORDER = (
        (0, 0, 0), (0, 1, 0), (1, 0, 0), (1, 1, 0), (0, 0, 1), (0, 1, 1), (1, 0, 1),
        (1, 1, 1), (0, 0, 2), (0, 1, 2), (1, 0, 2), (1, 1, 2), (0, 0, 3), (1, 0, 3),
    )

    def piece(way, slot, extra):
        kind, half, hops = ORDER[slot]
        hops = hops + extra
        zs = (z + (NZ - hops if way == 0 else hops)) % NZ
        return kind, weights.at[kind, zs, c, pl.ds((half ^ way) * 128, 128), :]

    def share(kind, ref):
        begin(remote(ref, ref, sib_send, sib_recv.at[kind], (sp, sib)))

    def ring_send_slot(slot):
        for way in range(2):
            to = ((z + (1 if way == 0 else NZ - 1)) % NZ) * NX + x
            _, ref = piece(way, slot, 0)
            begin(remote(ref, ref, ring_send, ring_recv.at[way, slot], (to, tp)))

    def ring_take(slot):
        for way in range(2):
            kind, ref = piece(way, slot, 1)
            arrival(ref, ring_recv.at[way, slot])
            share(kind, ref)

    own_block = pl.ds(pl.multiple_of(inner * TOK, TOK), TOK)

    def plane(off):
        to = (chip + off) % (NX * NY)
        return (z * NX + to // NY, (to % NY) * 2 + block)

    def to_plane(src, dst, send, recv):
        @pl.loop(1, NX * NY)
        def _(off):
            remote(src, dst, send.at[0], recv, plane(off)).start()

        @pl.when(c == block)
        def _():
            pltpu.make_async_copy(src, dst, recv).start()

        @pl.when(c != block)
        def _():
            remote(src, dst, send.at[1], recv, plane(0)).start()

    def plane_sent(src, dst, send, recv, fifteen):
        arrival(fifteen, send.at[0])

        @pl.when(c != block)
        def _():
            remote(src, dst, send.at[1], recv, plane(0)).wait_send()

    res_dst = res_v.at[own_block, pl.ds(pl.multiple_of(tp * 256, 256), 256)]
    build_maps(1)

    arrival(weights.at[0, z, c], up_recv)
    ring_send_slot(0)
    share(0, weights.at[0, z, c])
    to_plane(residual, res_dst, res_send, res_recv)

    arrival(cx.at[pl.ds(0, NX - 1)], cx_recv)

    def as_map(ref, n, top):
        return tuple(ref[n, top + q : top + q + 1, :] for q in range(4))

    row = []
    for e in range(2):
        run = unit
        for n in range(NX) if e == 0 else reversed(range(NX)):
            run = composed(run, as_map(cx, n, 4 * e))
        row += list(run)
    row_ends[0] = jnp.concatenate(row[:4], axis=0)
    row_ends[1] = jnp.concatenate(row[4:], axis=0)
    cz[z] = jnp.concatenate(row[:4], axis=0)
    for off in (4, 3, 5, 2, 6, 1, 7):
        copy = remote(
            row_ends.at[jnp.where(z + off < NZ, 0, 1)], cz.at[z], cz_send, cz_recv,
            (((z + off) % NZ) * NX + x, tp),
        )
        copy.start()

    ring_send_slot(1)
    arrival(weights.at[1, z, c], down_recv)
    ring_send_slot(2)
    ring_send_slot(3)
    share(1, weights.at[1, z, c])
    ring_take(0)
    ring_send_slot(4)
    ring_take(1)
    ring_send_slot(5)

    arrival(cz.at[pl.ds(0, NZ - 1)], cz_recv)
    ring_take(2)
    ring_send_slot(6)

    def applied(m, state):
        pre, pim, hre, him = m
        re, im = state
        return pre * re - pim * im + hre, pre * im + pim * re + him

    blank = jnp.zeros((1, ST), F32)
    out_y = jnp.zeros((TOK, CH), F32)
    for e in range(2):
        state = (blank, blank)
        for ref, count, at, top in ((cz, NZ, z, 0), (cx, NX, x, 4 * e)):
            for n in range(count) if e == 0 else reversed(range(count)):
                passed = (n < at) if e == 0 else (n > at)
                new = applied(as_map(ref, n, top), state)
                state = tuple(jnp.where(passed, a, b) for a, b in zip(new, state))
        entry = applied(before[e], state)
        tall = tuple(jnp.concatenate([v] * STEPS, axis=0) for v in entry)
        pre, pim = prefix_s[e, 0], prefix_s[e, 1]
        re = state_s[e, 0] + pre * tall[0] - pim * tall[1]
        im = state_s[e, 1] + pre * tall[1] + pim * tall[0]
        for part, value in ((0, re), (1, -im)):
            high, low = halves(value)
            out_y = out_y + nt(high, maps_v[e, 1, part, 0])
            out_y = out_y + (nt(low, maps_v[e, 1, part, 0]) + nt(high, maps_v[e, 1, part, 1]))

    mine = iota((8, CH), 0) == tp
    skip_row = jnp.sum(jnp.where(mine, skip_v[...], 0.0), axis=0, keepdims=True)
    closing_row = jnp.sum(jnp.where(mine, closing_v[...], 0.0), axis=0, keepdims=True)
    v = out_y + skip_row * lifted_s[...]
    act = 0.5 * v * (1.0 + jnp.tanh(0.7978845608028654 * (v + 0.044715 * v * v * v)))
    act = act * lax.rsqrt(jnp.mean(act * act, axis=1, keepdims=True) + EPSILON) * closing_row
    merged_v[...] = mm(perm_back.astype(BF16), act.astype(BF16)).astype(BF16)
    mg_dst = gathered.at[own_block, pl.ds(pl.multiple_of(tp * CH, CH), CH)]
    to_plane(merged_v, mg_dst, mg_send, mg_recv)

    ring_take(3)
    ring_send_slot(7)
    ring_take(4)
    ring_send_slot(8)
    ring_take(5)
    ring_send_slot(9)
    ring_take(6)
    ring_send_slot(10)
    ring_take(7)
    ring_send_slot(11)
    ring_take(8)
    ring_send_slot(12)
    ring_take(9)
    ring_take(10)
    ring_send_slot(13)
    ring_take(11)
    copies[-1].wait()
    copies[-2].wait()
    arrival(res_v, res_recv)
    arrival(gathered, mg_recv)

    def project(n, squares):
        cols = pl.ds(n * 1024, 1024)
        m = mm(gathered[...], emitted_v[:, cols]) + res_v[:, cols].astype(F32)
        mid_f[:, cols] = m
        mid_v[:, cols] = (m * leading_v[:, cols]).astype(BF16)
        return squares + jnp.sum(m * m, axis=1, keepdims=True)

    squares = project(0, jnp.zeros((2 * TOK, 1), F32))
    ring_take(12)
    squares = project(1, squares)
    scale = lax.rsqrt(squares * (1.0 / D) + EPSILON)

    own_cols = pl.ds(pl.multiple_of(tp * 256, 256), 256)
    sib_cols = pl.ds(pl.multiple_of(sib * 256, 256), 256)

    @pl.when(c == block)
    def _():
        remote(mid_f.at[own_block, sib_cols], own_mid, mid_send, mid_recv, (sp, sib)).start()

    ring_take(13)
    arrival(weights.at[0, :, 1 - c], sib_recv.at[0])
    for n in range(2):
        up = mm(mid_v[...], weights[0, :, n].reshape(D, 256)) * scale
        up = jnp.maximum(up, 0.0)
        hidden[:, n * 256 : (n + 1) * 256] = (up * up).astype(BF16)
    arrival(weights.at[1, :, 1 - c], sib_recv.at[1])

    def down(*ns):
        both = [nt(hidden[:, :256], weights[1, n, 0]) + nt(hidden[:, 256:], weights[1, n, 1]) for n in ns]
        for n, value in zip(ns, both):
            partial[n] = value.astype(BF16)

    def row_of(k):
        return (y + 1 + k) % NY

    def along_y(i, k):
        to = row_of(k)
        src = partial.at[2 * to + 1, pl.ds(i * TOK, TOK), :]
        dst = from_y.at[i, y]
        return src, dst, remote(src, dst, ay_send, ay_recv.at[i], (sp, 2 * to + c))

    def along_x(k, i):
        src = partial.at[2 * row_of(k), pl.ds(i * TOK, TOK), :]
        dst = from_x.at[row_of(k), x]
        to = (z * NX + 2 * c + i, tp)
        return src, dst, remote(src, dst, ax_send, ax_recv.at[k], to)

    def on_y(i):
        dst = final.at[x]
        to = (z * NX + 2 * c + i, y * 2 + 1)
        return sum_y.at[i], dst, remote(sum_y.at[i], dst, fy_send.at[i], final_recv, to)

    def on_x(k):
        dst = final.at[y]
        to = (sp, row_of(k) * 2)
        return sum_x.at[k], dst, remote(sum_x.at[k], dst, fx_send.at[k], final_recv, to)

    def deliver(triple, recv, local):
        src, dst, copy = triple
        if local is None:
            copy.start()
            return

        @pl.when(local)
        def _():
            pltpu.make_async_copy(src, dst, recv).start()

        @pl.when(jnp.logical_not(local))
        def _():
            copy.start()

    def delivered(triple, local):
        if local is None:
            triple[2].wait_send()
            return

        @pl.when(jnp.logical_not(local))
        def _():
            triple[2].wait_send()

    def near(i):
        return (2 * c + i) == x

    def local_y(k):
        return (c == 0) if k == NY - 1 else None

    for k in (1, 0, 2, 3):
        down(2 * row_of(k) + 1, 2 * row_of(k))
        if k < NY - 1:
            along_y(0, k)[2].start()
        else:
            for i in range(2):
                src, dst, _ = along_y(i, k)
                pltpu.make_async_copy(src, dst, ay_recv.at[i]).start()
        for i in range(2):
            deliver(along_x(k, i), ax_recv.at[k], near(i))
        if k == 2:
            for n in (1, 0, 2):
                along_y(1, n)[2].start()

    def summed(ref):
        total = ref[0].astype(F32)
        for n in range(1, NX):
            total = total + ref[n].astype(F32)
        return total

    def turn_x(k):
        @pl.when(c == block)
        def _():
            arrival(from_x.at[row_of(k)], ax_recv.at[k])
            sum_x[k] = summed(from_x.at[row_of(k)]).astype(BF16)
            deliver(on_x(k), final_recv, local_y(k))

    def turn_y(i):
        arrival(from_y.at[i], ay_recv.at[i])
        sum_y[i] = summed(from_y.at[i]).astype(BF16)
        deliver(on_y(i), final_recv, jnp.logical_and(near(i), c == 1))

    @pl.when(c == block)
    def _():
        own_mid_copy = pltpu.make_async_copy(mid_f.at[own_block, own_cols], own_mid, mid_recv)
        own_mid_copy.start()

    turn_x(1)
    turn_x(0)
    turn_x(2)
    turn_x(3)
    turn_y(0)
    turn_y(1)

    arrival(hidden.at[pl.ds(0, 192), :], up_send)
    arrival(cx.at[pl.ds(0, NX - 1)], cx_send)
    arrival(cz.at[pl.ds(0, NZ - 1)], cz_send)
    arrival(weights.at[0, pl.ds(0, 7)], ring_send)
    arrival(weights.at[0], sib_send)
    plane_sent(residual, res_dst, res_send, res_recv, res_v.at[pl.ds(0, 240), :])
    plane_sent(merged_v, mg_dst, mg_send, mg_recv, gathered.at[pl.ds(0, 240), :])

    @pl.when(c == block)
    def _():
        remote(mid_f.at[own_block, sib_cols], own_mid, mid_send, mid_recv, (sp, sib)).wait_send()

    arrival(own_mid, mid_recv)
    arrival(final, final_recv)
    out[...] = (own_mid[...] + summed(final)).astype(BF16)

    arrival(partial.at[pl.ds(0, 3)], ay_send)

    @pl.when(c == block)
    def _():
        arrival(partial.at[pl.ds(0, 2)], ax_send)
        for k in range(NY):
            delivered(on_x(k), local_y(k))

    @pl.when(c != block)
    def _():
        arrival(partial.at[pl.ds(0, 4)], ax_send)

    for i in range(2):
        delivered(on_y(i), jnp.logical_and(near(i), c == 1))


def on_device(
    residual, lifted, pace, fading, rate_l, rate_s, turn_l, turn_s, proj_l, proj_s,
    skip, closing, emitted, leading, raising, lowering,
):
    dma = pltpu.SemaphoreType.DMA
    vm = pltpu.VMEM
    return pl.pallas_call(
        kernel,
        out_shape=pltpu.VMEM((TOK, 256), BF16),
        in_specs=[pl.BlockSpec(memory_space=pl.ANY)] * 16,
        out_specs=pl.BlockSpec(memory_space=pltpu.VMEM),
        scratch_shapes=[
            vm((TOK, CH), BF16), vm((8, TOK), F32), vm((8, TOK), F32),
            vm((2, 32, 64), F32), vm((2, 32, 32), F32), vm((2, 32, 64), F32), vm((2, 32, 32), F32),
            vm((2, 2, 2, 4, 16, 64), F32), vm((2, 2, 2, 4, 16, 32), F32),
            vm((8, CH), F32), vm((8, CH), F32), vm((64, 1024), BF16), vm((64, 1024), BF16), vm((1024, D), BF16), vm((1, D), F32),
            vm((2, 2, 2, 2, CH, ST), BF16), vm((TOK, ST), F32), vm((TOK, ST), F32),
            vm((2, 2, TOK, ST), F32), vm((2, 2, TOK, ST), F32), vm((2, 2, TOK, ST), F32),
            vm((TOK, CH), F32),
            vm((8, ST), F32), vm((NX, 8, ST), F32), vm((NZ, 4, ST), F32), vm((2, 4, ST), F32),
            vm((TOK, CH), BF16), vm((2 * TOK, 1024), BF16), vm((2 * TOK, D), BF16),
            vm((2 * TOK, D), BF16), vm((2 * TOK, D), F32), vm((TOK, 256), F32),
            vm((2, NZ, 2, 256, 256), BF16), vm((2 * TOK, 512), BF16),
            vm((8, 2 * TOK, 256), BF16), vm((2, NY, TOK, 256), BF16), vm((NY, NX, TOK, 256), BF16),
            vm((2, TOK, 256), BF16), vm((NY, TOK, 256), BF16), vm((4, TOK, 256), BF16),
            dma((15,)), dma, dma, dma, dma, dma, dma, dma,
            dma((2,)), dma, dma, dma((2,)), dma, dma((4,)), dma((2,)), dma((4,)), dma,
            dma((2,)), dma, dma, dma((2, 14)), dma, dma((2,)), dma, dma,
        ],
        compiler_params=pltpu.CompilerParams(
            collective_id=0, has_side_effects=True, vmem_limit_bytes=60 * 1024 * 1024
        ),
        name="layer",
    )(
        residual, lifted, pace, fading, rate_l, rate_s, turn_l, turn_s,
        proj_l.swapaxes(-1, -2), proj_s.swapaxes(-1, -2),
        skip.reshape(8, CH), closing.reshape(8, CH), emitted, leading.reshape(1, D), raising, lowering.T,
    )


def solution(mesh):
    rest = [P()] * 10
    return jax.shard_map(
        on_device,
        mesh=mesh,
        in_specs=(P("sp", "tp"), P("sp", "tp"), P("tp", "sp"), P("tp", "sp"), *rest, P("sp", "tp"), P("tp", "sp")),
        out_specs=P("sp", "tp"),
        check_vma=False,
    )
```
